256 devices in a mesh: sp: 64 (over z, x, core), tp: 4 (over y).
Axes of the slice: x: 4, y: 4, z: 8, core: 2. Of those that a mesh axis runs over, the one named last changes fastest.
Arguments:
- hidden_in: bfloat16 [16384, 2048], P('sp'), may hold values from -6 to 6
- cotangent: bfloat16 [16384, 2048], P('sp'), may hold values from -16 to 16
- routes: int32 [16384, 2], P('sp'), may hold values from 0 to 63, all different within a row; in each aligned block of 256 rows (0 to 255, 256 to 511, ...) at most 12 rows name the same one
- routing_weights: float32 [16384, 2], P('sp'), may hold values from 0.1 to 1
- w_gate: bfloat16 [64, 2048, 1024], P('sp', None, 'tp'), may hold values from -0.125 to 0.125
- w_up: bfloat16 [64, 2048, 1024], P('sp', None, 'tp'), may hold values from -0.125 to 0.125
- w_down: bfloat16 [64, 1024, 2048], P('sp', 'tp'), may hold values from -0.1875 to 0.1875
- b_gate: bfloat16 [16384, 1024], P('sp', 'tp'), may hold values from -6 to 6
- c_gate: bfloat16 [16384, 1024], P('sp', 'tp'), may hold values from -6 to 6
- x_in: bfloat16 [16384, 1024], P('sp', 'tp'), may hold values from -6 to 6
- taps: bfloat16 [3, 1024], P(None, 'tp'), may hold values from -3 to 3
- w_out: bfloat16 [2048, 1024], P(None, 'tp'), may hold values from -0.1875 to 0.1875
Outputs:
- grad_gate: bfloat16 [64, 2048, 1024], P('sp', None, 'tp')
- grad_up: bfloat16 [64, 2048, 1024], P('sp', None, 'tp')
- grad_down: bfloat16 [64, 1024, 2048], P('sp', 'tp')
- out_proj_grad: float32 [2048, 1024], P('sp', 'tp')
- residual_grad: bfloat16 [16384, 2048], P('sp', 'tp')
- grad_b: bfloat16 [16384, 1024], P('sp', 'tp')
- grad_c: bfloat16 [16384, 1024], P('sp', 'tp')
- grad_x: bfloat16 [16384, 1024], P('sp', 'tp')
The draws below stay inside these ranges and needn't reach their ends.
Inputs may be any that keep to these rules, and one draw needn't show every extreme that they name: `routes`: each row names 2 different experts. Among the rows of one index of sp no expert is named more than 12 times, a bound that some block reaches in some of them.
All inputs are finite; a program needn't handle non-finite values.
Results may differ from the reference program's by a relative error of at most 0.01.
Values may be sent and summed in bfloat16 or wider, within the bound.
A program may use at most 64 MiB of HBM per device.

```python
import math
import jax
import jax.numpy as jnp
import numpy as np
from jax import lax

D = 2048
SHORT = 1024
FF = 1024
TOP = 2
TOK_DEV = 256
EXPERTS = 64
CAP = 12
TOKENS = 16384
N_SP = 64
N_TP = 4


def spiked(entries, key, source, target, blocks, factor):
    owner, partner = [(jnp.arange(entries.shape[dim]) // (entries.shape[dim] // blocks)).reshape([-1 if axis == dim else 1 for axis in range(entries.ndim)]) for dim in (source, target)]
    chosen = jax.random.permutation(key, blocks)[partner]
    strong = (owner == chosen) | (owner == (partner + blocks // 2) % blocks)
    return jnp.where(strong, factor * entries, entries)


def shard_levels(own_key, shape, cuts, smallest, largest):
    def one(dim, shards_of):
        heights = jax.random.uniform(jax.random.fold_in(jax.random.fold_in(own_key, 6), dim), (shards_of,), jnp.float32, smallest / len(cuts), largest / len(cuts))
        return jnp.repeat(jnp.exp(heights), shape[dim] // shards_of).reshape((-1,) + (1,) * (len(shape) - dim - 1))

    factor_of = one(*cuts[0])
    for cut in cuts[1:]:
        factor_of = factor_of * one(*cut)
    return factor_of


def routed_block(rng, own, number, rows, amount, top, bound, skew):
    order = jax.random.permutation(rng, amount)
    crowded, ordinary = load_shares(amount, rows * top, bound, skew, True), load_shares(amount, rows * top, bound, skew, False)
    places = jnp.arange(amount)

    def named(sizes, rotation):
        used = int((sizes > 0).sum())
        fixed = max(1, used // 4)
        passed = fixed + (places - fixed + rotation * (used - fixed)) % max(1, amount - fixed)
        return jnp.zeros((amount,), jnp.int32).at[order[jnp.where(places < fixed, places, passed)]].set(jnp.asarray(sizes, jnp.int32))

    sizes = jnp.where(number % 4 == 0, named(crowded, number // 4), named(ordinary, number - number // 4 - 1))
    mixed = jax.random.permutation(jax.random.fold_in(own, 3), amount)
    donor, receiver = mixed[0:amount // 2 * 2:2], mixed[1:amount // 2 * 2:2]
    room = jnp.minimum(sizes[donor] - 1, bound - sizes[receiver]) // 2
    room = jnp.where((donor == order[0]) | (receiver == order[0]) | (sizes[receiver] == 0), 0, jnp.maximum(room, 0))
    passed = jax.random.randint(jax.random.fold_in(own, 4), (amount // 2,), 0, 1 << 20) % (room + 1)
    sizes = sizes.at[donor].add(-passed).at[receiver].add(passed)
    members = jnp.searchsorted(jnp.cumsum(sizes), jnp.arange(rows * top), side="right").astype(jnp.int32)
    table = members.reshape(top, rows).T
    table = table[jax.random.permutation(jax.random.fold_in(own, 1), rows)]
    rotation = jax.random.randint(jax.random.fold_in(own, 2), (rows, 1), 0, top)
    return jnp.take_along_axis(table, (jnp.arange(top)[None, :] + rotation) % top, axis=1)


def load_shares(number_of, total, bound, slope, full):
    weights = [(1 << 20) // math.isqrt(grade ** slope) + 1 for grade in range(1, number_of + 1)]
    largest = bound if full else min(bound, max(-(-total // number_of), total * weights[0] // sum(weights)))
    least = 1 if total - largest >= number_of - 1 else 0
    given, rest = [largest] + [least] * (number_of - 1), total - largest - least * (number_of - 1)
    while rest > 0:
        candidates = [i for i in range(1, number_of) if given[i] < largest] or [i for i in range(1, number_of) if given[i] < bound]
        mass, left = sum([weights[i] for i in candidates]), rest
        for i in candidates:
            more = min(bound - given[i], max(1, left * weights[i] // mass), rest)
            given[i] = given[i] + more
            rest = rest - more
    return np.array(given)


def bell_draw(key, dims, spread, limit, cuts=(), kind=jnp.bfloat16):
    entries = spread * jax.random.normal(key, dims, jnp.float32)
    if cuts:
        entries = entries * shard_levels(key, dims, cuts, -0.22, 0.18)
    return jnp.clip(entries, -limit, limit).astype(kind)


def noise_with(key, dims, deviation, limit, shards, heavy, kind=jnp.bfloat16):
    array = deviation * jax.random.normal(key, dims, jnp.float32)
    if shards:
        array = array * shard_levels(key, dims, shards, -0.22, 0.18)
    return jnp.clip(spiked(array, jax.random.fold_in(key, 3), *heavy), -limit, limit).astype(kind)


def setup_inputs(seed: int = 0) -> dict:
    streams_of = jax.random.split(jax.random.key(seed), 13)
    hidden_in = bell_draw(streams_of[0], (TOKENS, D), 1.0, 6.0, ((0, 64),))
    cotangent = noise_with(streams_of[1], (TOKENS, D), 1.0, 16.0, ((0, 64),), (0, 1, 64, 4.0))
    routes_keys = jax.random.split(jax.random.fold_in(streams_of[2], 1), TOKENS // TOK_DEV)
    routes_turns = jax.random.permutation(jax.random.fold_in(streams_of[2], 3), TOKENS // TOK_DEV)
    routes = jax.vmap(lambda own, number: routed_block(jax.random.fold_in(streams_of[2], 2), own, number, TOK_DEV, EXPERTS, TOP, CAP, 1))(routes_keys, routes_turns).reshape((TOKENS, TOP))
    routing_weights = jnp.clip(jnp.exp(math.log(1.0) - 2.3025851 * jax.random.uniform(streams_of[3], (TOKENS, TOP), jnp.float32) ** shard_levels(streams_of[3], (TOKENS, TOP), ((0, 64),), -0.2, 0.2)), 0.1, 1.0)
    w_gate = bell_draw(streams_of[4], (EXPERTS, D, FF), D ** -0.5, 0.125, ((0, 64), (2, 4)))
    w_up = bell_draw(streams_of[5], (EXPERTS, D, FF), D ** -0.5, 0.125, ((0, 64), (2, 4)))
    w_down = bell_draw(streams_of[6], (EXPERTS, FF, D), FF ** -0.5, 0.1875, ((0, 64), (1, 4)))
    b_gate = bell_draw(streams_of[7], (TOKENS, SHORT), 1.0, 6.0, ((0, 64), (1, 4)))
    c_gate = bell_draw(streams_of[8], (TOKENS, SHORT), 1.0, 6.0, ((0, 64), (1, 4)))
    x_in = bell_draw(streams_of[9], (TOKENS, SHORT), 1.0, 6.0, ((0, 64), (1, 4)))
    taps = bell_draw(streams_of[10], (3, SHORT), 0.6, 3.0, ((1, 4),))
    w_out = bell_draw(streams_of[11], (D, SHORT), SHORT ** -0.5, 0.1875, ((1, 4),))
    return {"hidden_in": hidden_in, "cotangent": cotangent, "routes": routes, "routing_weights": routing_weights, "w_gate": w_gate, "w_up": w_up, "w_down": w_down, "b_gate": b_gate, "c_gate": c_gate, "x_in": x_in, "taps": taps, "w_out": w_out}


def reference(hidden_in, cotangent, routes, routing_weights, w_gate, w_up, w_down, b_gate, c_gate, x_in, taps, w_out):
    flat_ids = routes.reshape(-1).astype(jnp.int32)
    flat_weights = routing_weights.reshape(-1).astype(jnp.float32)
    rows_each = N_SP * CAP
    part_width = FF // N_TP

    def one_expert(args):
        expert_id, gate_mat, up_mat, down_mat = args
        chosen = flat_ids == expert_id
        picked = jnp.nonzero(chosen, size=rows_each, fill_value=0)[0].astype(jnp.int32)
        filled = jnp.arange(rows_each, dtype=jnp.int32) < jnp.sum(chosen.astype(jnp.int32))
        token_of = picked // TOP
        rows_h = jnp.where(filled[:, None], hidden_in[token_of], jnp.zeros((), jnp.bfloat16))
        scaled = jnp.where(filled, flat_weights[picked], 0.0)
        rows_s = (scaled[:, None] * cotangent[token_of].astype(jnp.float32)).astype(jnp.bfloat16)
        pre_gate = jnp.dot(rows_h, gate_mat, preferred_element_type=jnp.float32)
        pre_up = jnp.dot(rows_h, up_mat, preferred_element_type=jnp.float32)
        sigma = jax.nn.sigmoid(pre_gate)
        silu_gate = pre_gate * sigma
        hid = (silu_gate * pre_up).astype(jnp.bfloat16)
        d_hid = jnp.dot(rows_s, down_mat.T, preferred_element_type=jnp.float32)
        d_up = (d_hid * silu_gate).astype(jnp.bfloat16)
        d_pre = (d_hid * pre_up * sigma * (1.0 + pre_gate * (1.0 - sigma))).astype(jnp.bfloat16)
        grad_down_e = jnp.dot(hid.T, rows_s, preferred_element_type=jnp.float32).astype(jnp.bfloat16)
        grad_gate_e = jnp.dot(rows_h.T, d_pre, preferred_element_type=jnp.float32).astype(jnp.bfloat16)
        grad_up_e = jnp.dot(rows_h.T, d_up, preferred_element_type=jnp.float32).astype(jnp.bfloat16)
        total = jnp.zeros((rows_each, D), jnp.float32)
        for block in range(N_TP):
            lower = block * part_width
            upper = lower + part_width
            partial_sum = jnp.dot(d_pre[:, lower:upper], gate_mat[:, lower:upper].T, preferred_element_type=jnp.float32)
            partial_sum = partial_sum + jnp.dot(d_up[:, lower:upper], up_mat[:, lower:upper].T, preferred_element_type=jnp.float32)
            total = total + partial_sum.astype(jnp.bfloat16).astype(jnp.float32)
        route_grad = jnp.where(filled[:, None], total.astype(jnp.bfloat16), jnp.zeros((), jnp.bfloat16))
        return grad_gate_e, grad_up_e, grad_down_e, route_grad, token_of

    expert_ids = jnp.arange(EXPERTS, dtype=jnp.int32)
    grad_gate, grad_up, grad_down, route_grads, token_ids = lax.map(one_expert, (expert_ids, w_gate, w_up, w_down))
    summed = jnp.zeros((TOKENS, D), jnp.float32).at[token_ids.reshape(-1)].add(route_grads.reshape(-1, D).astype(jnp.float32))
    residual_grad = (cotangent.astype(jnp.float32) + summed).astype(jnp.bfloat16)

    taps_f = taps.astype(jnp.float32)
    gated = c_gate.astype(jnp.float32) * x_in.astype(jnp.float32)
    padded = jnp.concatenate([jnp.zeros((2, SHORT), jnp.float32), gated], axis=0)
    conv = taps_f[0] * padded[0:TOKENS] + taps_f[1] * padded[1:TOKENS + 1] + taps_f[2] * padded[2:TOKENS + 2]
    b_f = b_gate.astype(jnp.float32)
    y_short = (b_f * conv).astype(jnp.bfloat16)
    d_y = jnp.dot(residual_grad, w_out, preferred_element_type=jnp.float32)
    grad_b = (d_y * conv).astype(jnp.bfloat16)
    d_conv = b_f * d_y
    later = jnp.concatenate([d_conv, jnp.zeros((2, SHORT), jnp.float32)], axis=0)
    d_v = taps_f[2] * later[0:TOKENS] + taps_f[1] * later[1:TOKENS + 1] + taps_f[0] * later[2:TOKENS + 2]
    grad_c = (d_v * x_in.astype(jnp.float32)).astype(jnp.bfloat16)
    grad_x = (d_v * c_gate.astype(jnp.float32)).astype(jnp.bfloat16)
    out_proj_grad = jnp.dot(residual_grad.T, y_short, preferred_element_type=jnp.float32)
    return grad_gate, grad_up, grad_down, out_proj_grad, residual_grad, grad_b, grad_c, grad_x
```

```python
import functools

import jax
import jax.numpy as jnp
from jax import lax
from jax.experimental import pallas as pl
from jax.experimental.pallas import tpu as pltpu
from jax.sharding import PartitionSpec as P

PLANES, PLANE, TP, CAP = 8, 8, 4, 12
SP = PLANES * PLANE
ROWS = 2 * CAP
VMEM = pl.BlockSpec(memory_space=pltpu.VMEM)
BF, F32 = jnp.bfloat16, jnp.float32


def dot(a, b, dims=((1,), (0,))):
    return lax.dot_general(a, b, (dims, ((), ())), preferred_element_type=F32)


def device(sp, tp):
    return {"sp": sp, "tp": tp}


def plane_step(g):
    return ((g + 1) // 2) * (2 * (g % 2) - 1)


def greet_all(me, y, right, left):
    barrier = pltpu.get_barrier_semaphore()

    def signal(i, c):
        pl.semaphore_signal(barrier, inc=1, device_id=device((me + i) % SP, y))
        return c

    lax.fori_loop(1, SP, signal, 0)
    pl.semaphore_signal(barrier, inc=1, device_id=device(me, right))
    pl.semaphore_signal(barrier, inc=1, device_id=device(me, left))
    return barrier


def wait_bytes(ref, sem):
    pltpu.make_async_copy(ref, ref, sem).wait()


def pack_kernel(routes, weights, hidden, cot, send, own, select):
    me, y = lax.axis_index("sp"), lax.axis_index("tp")
    tokens, width = hidden.shape
    share = width // TP
    down = lax.broadcasted_iota(jnp.int32, (tokens, tokens), 0)
    across = lax.broadcasted_iota(jnp.int32, (tokens, tokens), 1)

    def as_row(column):
        return jnp.sum(
            jnp.where(down == across, column, jnp.zeros_like(column)), axis=0, keepdims=True
        )

    def count(match):
        return jnp.sum(jnp.where(match, 1.0, 0.0), axis=0, keepdims=True).astype(jnp.int32)

    c0, c1 = routes[:, 0:1], routes[:, 1:2]
    r0, r1 = as_row(c0), as_row(c1)
    w0, w1 = as_row(weights[:, 0:1]), as_row(weights[:, 1:2])
    earlier = down < across
    t0 = r0 * ROWS + count(earlier & (c0 == r0))
    t1 = r1 * ROWS + count(c0 == r1) + count(earlier & (c1 == r1))
    part = PLANE * ROWS
    row = lax.broadcasted_iota(jnp.int32, (part, tokens), 0)
    is_token_row = lax.broadcasted_iota(jnp.int32, (part, 1), 0) % ROWS < CAP

    def picks(g):
        slot = row + g * part
        h = jnp.where((t0 == slot) | (t1 == slot), 1.0, 0.0)
        s0, s1 = t0 + CAP == slot, t1 + CAP == slot
        s = jnp.where(s0 | s1, 1.0, 0.0)
        scale = jnp.sum(jnp.where(s0, w0, 0.0) + jnp.where(s1, w1, 0.0), axis=1, keepdims=True)
        return h.astype(BF), s.astype(BF), (h + s).astype(BF), jnp.where(is_token_row, 1.0, scale)

    mine = pl.ds(pl.multiple_of(y * share, share), share)

    def one(g, c):
        h, s, both, scale = picks(g)
        rows = (dot(h, hidden[:, mine]) + dot(s, cot[:, mine])) * scale
        send[pl.ds(g * PLANE, PLANE)] = rows.astype(BF).reshape(PLANE, ROWS, share)
        select[pl.ds(pl.multiple_of(g * part, part), part), :] = both
        return c

    lax.fori_loop(0, PLANES, one, 0)
    h, s, _, scale = picks(me // PLANE)
    for k in range(TP):
        cols = pl.ds(k * share, share)
        rows = (dot(h, hidden[:, cols]) + dot(s, cot[:, cols])) * scale
        own[k] = rows.astype(BF).reshape(PLANE, ROWS, share)


def pack(routes, weights, hidden, cot):
    tokens, width = hidden.shape
    share = width // TP
    return pl.pallas_call(
        pack_kernel,
        out_shape=(
            jax.ShapeDtypeStruct((SP, ROWS, share), BF),
            jax.ShapeDtypeStruct((TP, PLANE, ROWS, share), BF),
            jax.ShapeDtypeStruct((SP * ROWS, tokens), BF),
        ),
        in_specs=[VMEM] * 4,
        out_specs=(VMEM,) * 3,
        compiler_params=pltpu.CompilerParams(vmem_limit_bytes=40 * 2**20),
        name="pack",
    )(routes, weights, hidden, cot)


def dispatch_kernel(send, own, got, z_in, z_out, f_in, f_out, y_in, y_out):
    me, y = lax.axis_index("sp"), lax.axis_index("tp")
    z, cell = me // PLANE, me % PLANE
    right, left, far = (y + 1) % TP, (y + 3) % TP, (y + 2) % TP
    barrier = greet_all(me, y, right, left)
    got[y, me] = send[me]
    for k in range(1, TP):
        got[(y + k) % TP, me] = own[(y + k) % TP, cell]
    pl.semaphore_wait(barrier, SP + 1)

    def send_block(i, c):
        g, j = i // PLANE, i % PLANE
        to = ((z + plane_step(g) + PLANES) % PLANES) * PLANE + (cell + j) % PLANE
        pltpu.make_async_remote_copy(
            send.at[to], got.at[y, me], z_out, z_in.at[g], device_id=device(to, y)
        ).start()
        return c

    lax.fori_loop(1, SP, send_block, 0)
    near = (TP - 1) * (PLANE - 1)

    def send_full(i, c):
        j, s = (cell + 1 + i % (PLANE - 1)) % PLANE, (y + 1 + i // (PLANE - 1)) % TP
        pltpu.make_async_remote_copy(
            own.at[s, j], got.at[s, me], f_out, f_in, device_id=device(z * PLANE + j, y)
        ).start()
        return c

    lax.fori_loop(0, near, send_full, 0)

    def block(s, g, at=0, size=PLANE):
        source = (z - plane_step(g) + PLANES) % PLANES
        return got.at[s, pl.ds(source * PLANE + at, size)]

    def pass_on(s, g, k, to):
        ref = block(s, g) if k < 2 else block(s, g, (k - 2) * (PLANE // 2), PLANE // 2)
        return pltpu.make_async_remote_copy(
            ref, ref, y_out.at[k], y_in.at[k, g], device_id=device(me, to)
        )

    def step(g, c):
        @pl.when(g < PLANES)
        def _():
            wait_bytes(block(y, g), z_in.at[g])
            pass_on(y, g, 0, right).start()
            pass_on(y, g, 1, left).start()

        @pl.when(g > 1)
        def _():
            pass_on(left, g - 1, 0, left).wait_recv()
            pass_on(left, g - 1, 2, right).start()
            pass_on(right, g - 1, 1, right).wait_recv()
            pass_on(right, g - 1, 3, left).start()

        return c

    lax.fori_loop(1, PLANES + 1, step, 0)

    def last(g, c):
        pass_on(far, g, 2, right).wait_recv()
        pass_on(far, g, 3, left).wait_recv()
        return c

    lax.fori_loop(1, PLANES, last, 0)
    for k in range(4):
        size = PLANE if k < 2 else PLANE // 2
        wait_bytes(got.at[0, pl.ds(0, size * (PLANES - 1))], y_out.at[k])
    wait_bytes(got.at[0, pl.ds(0, PLANE - 1)], z_in.at[0])
    wait_bytes(got.at[0, pl.ds(0, near)], f_in)
    wait_bytes(got.at[0, pl.ds(0, near)], f_out)
    wait_bytes(got.at[0, pl.ds(0, SP - 1)], z_out)


def dispatch(send, own):
    dma = pltpu.SemaphoreType.DMA
    return pl.pallas_call(
        dispatch_kernel,
        out_shape=jax.ShapeDtypeStruct((TP, *send.shape), BF),
        in_specs=[VMEM] * 2,
        out_specs=VMEM,
        scratch_shapes=[dma((PLANES,)), dma(()), dma(()), dma(()), dma((4, PLANES)), dma((4,))],
        compiler_params=pltpu.CompilerParams(
            collective_id=0, has_side_effects=True, vmem_limit_bytes=40 * 2**20
        ),
        name="dispatch",
    )(send, own)


def expert_kernel(got, w_gate, w_up, w_down, part, d_pre_out, d_up_out, hid_out):
    share, hidden = got.shape[3], w_gate.shape[1]
    rows = PLANE * ROWS
    is_token = lax.broadcasted_iota(jnp.int32, (rows, 1), 0) % ROWS < CAP

    def one(g, c):
        blocks = pl.ds(g * PLANE, PLANE)
        pre_gate = pre_up = d_hid = jnp.zeros((rows, hidden), F32)
        for k in range(TP):
            x = got[k, blocks].reshape(rows, share)
            cols = pl.ds(k * share, share)
            pre_gate += dot(x, w_gate[cols, :])
            pre_up += dot(x, w_up[cols, :])
            d_hid += dot(x, w_down[:, cols], ((1,), (1,)))
        d_hid = pltpu.roll(d_hid, rows - CAP, 0)
        sigma = 1.0 / (1.0 + jnp.exp(-pre_gate))
        silu = pre_gate * sigma
        hid = silu * pre_up
        d_up = d_hid * silu
        d_pre = d_hid * pre_up * sigma * (1.0 + pre_gate * (1.0 - sigma))
        at = pl.ds(pl.multiple_of(g * rows, rows), rows)
        d_pre_out[at, :] = jnp.where(is_token, d_pre, 0.0).astype(BF)
        d_up_out[at, :] = jnp.where(is_token, d_up, 0.0).astype(BF)
        hid_out[at, :] = jnp.where(is_token, 0.0, pltpu.roll(hid, CAP, 0)).astype(BF)
        twice_pre = jnp.where(is_token, d_pre, pltpu.roll(d_pre, CAP, 0)).astype(BF)
        twice_up = jnp.where(is_token, d_up, pltpu.roll(d_up, CAP, 0)).astype(BF)
        for k in range(TP):
            cols = pl.ds(k * share, share)
            grad = dot(twice_pre, w_gate[cols, :], ((1,), (1,)))
            grad += dot(twice_up, w_up[cols, :], ((1,), (1,)))
            half = share // 2
            folded = jnp.where(is_token, grad[:, :half], grad[:, half:])
            part[k, blocks] = folded.astype(BF).reshape(PLANE, ROWS, half)
        return c

    lax.fori_loop(0, PLANES, one, 0)


def experts(got, w_gate, w_up, w_down):
    share, hidden = got.shape[3], w_gate.shape[1]
    flat = jax.ShapeDtypeStruct((SP * ROWS, hidden), BF)
    return pl.pallas_call(
        expert_kernel,
        out_shape=(jax.ShapeDtypeStruct((TP, SP, ROWS, share // 2), BF), flat, flat, flat),
        in_specs=[VMEM] * 4,
        out_specs=(VMEM,) * 4,
        compiler_params=pltpu.CompilerParams(vmem_limit_bytes=50 * 2**20),
        name="experts",
    )(got, w_gate, w_up, w_down)


def return_kernel(part, back, near_in, total_in, sums, a_in, a_out, b_in, b_out, z_in, z_out):
    me, y = lax.axis_index("sp"), lax.axis_index("tp")
    z, cell = me // PLANE, me % PLANE
    right, left, far = (y + 1) % TP, (y + 3) % TP, (y + 2) % TP
    half = PLANE // 2
    pl.semaphore_wait(greet_all(me, y, right, left), SP + 1)

    def source(i):
        return (z + plane_step(PLANES - 1 - i) + PLANES) % PLANES

    def far_half(i, k, to):
        at = source(i) * PLANE + k * half
        return pltpu.make_async_remote_copy(
            part.at[far, pl.ds(at, half)],
            near_in.at[k, i],
            a_out.at[k],
            a_in.at[k, i],
            device_id=device(me, to),
        )

    def near_sum(i, k, to):
        return pltpu.make_async_remote_copy(
            part.at[to, pl.ds(source(i) * PLANE, PLANE)],
            total_in.at[k, i],
            b_out.at[k],
            b_in.at[k, i],
            device_id=device(me, to),
        )

    def start(i, c):
        far_half(i, 0, right).start()
        far_half(i, 1, left).start()
        return c

    def add(i, k, to):
        at = pl.ds(source(i) * PLANE + k * half, half)
        part[to, at] = (part[to, at].astype(F32) + near_in[k, i].astype(F32)).astype(BF)

    def send_back(i, j):
        to = source(i) * PLANE + (cell + j) % PLANE
        pltpu.make_async_remote_copy(
            sums.at[to], back.at[me], z_out, z_in, device_id=device(to, y)
        ).start()

    lax.fori_loop(0, 2, start, 0)

    def step(i, c):
        @pl.when(i < PLANES)
        def _():
            far_half(i, 0, right).wait_recv()
            add(i, 0, right)
            far_half(i, 1, left).wait_recv()
            add(i, 1, left)

            @pl.when(i + 2 < PLANES)
            def _():
                start(i + 2, 0)

            near_sum(i, 0, right).start()
            near_sum(i, 1, left).start()

        @pl.when(i > 0)
        def _():
            p = i - 1
            near_sum(p, 0, right).wait_recv()
            near_sum(p, 1, left).wait_recv()
            at = pl.ds(source(p) * PLANE, PLANE)
            sums[at] = (
                part[y, at].astype(F32) + total_in[0, p].astype(F32) + total_in[1, p].astype(F32)
            ).astype(BF)

            @pl.when(p < PLANES - 1)
            def _():
                send_back(p, 0)

            lax.fori_loop(1, PLANE, lambda j, d: (send_back(p, j), d)[1], 0)

        return c

    lax.fori_loop(0, PLANES + 1, step, 0)
    back[me] = sums[me]
    for k in range(2):
        wait_bytes(part.at[0, pl.ds(0, SP // 2)], a_out.at[k])
        wait_bytes(part.at[0], b_out.at[k])
    wait_bytes(part.at[0, pl.ds(0, SP - 1)], z_in)
    wait_bytes(part.at[0, pl.ds(0, SP - 1)], z_out)


def return_rows(part):
    dma = pltpu.SemaphoreType.DMA
    rows, half = part.shape[2:]
    return pl.pallas_call(
        return_kernel,
        out_shape=jax.ShapeDtypeStruct((SP, rows, half), BF),
        in_specs=[VMEM],
        out_specs=VMEM,
        scratch_shapes=[
            pltpu.VMEM((2, PLANES, PLANE // 2, rows, half), BF),
            pltpu.VMEM((2, PLANES, PLANE, rows, half), BF),
            pltpu.VMEM((SP, rows, half), BF),
            dma((2, PLANES)),
            dma((2,)),
            dma((2, PLANES)),
            dma((2,)),
            dma(()),
            dma(()),
        ],
        input_output_aliases={},
        compiler_params=pltpu.CompilerParams(
            collective_id=1, has_side_effects=True, vmem_limit_bytes=40 * 2**20
        ),
        name="return_rows",
    )(part)


def combine_kernel(select, back, cot, full, y_in, y_out):
    me, y = lax.axis_index("sp"), lax.axis_index("tp")
    right, left, far = (y + 1) % TP, (y + 3) % TP, (y + 2) % TP
    tokens, share = full.shape[1:]
    half = share // 2
    barrier = pltpu.get_barrier_semaphore()
    pl.semaphore_signal(barrier, inc=1, device_id=device(me, right))
    pl.semaphore_signal(barrier, inc=1, device_id=device(me, left))
    slots = SP * ROWS
    is_token = lax.broadcasted_iota(jnp.int32, (slots, 1), 0) % ROWS < CAP
    rows = back[...].reshape(slots, half)
    zero = jnp.zeros_like(rows)
    for k, kept in enumerate((jnp.where(is_token, rows, zero), jnp.where(is_token, zero, rows))):
        cols = pl.ds(pl.multiple_of(y * share + k * half, half), half)
        total = cot[:, cols].astype(F32) + dot(select[...], kept, ((0,), (0,)))
        full[y, :, pl.ds(k * half, half)] = total.astype(BF)
    pl.semaphore_wait(barrier, 2)

    def pass_on(s, k, to):
        ref = full.at[s] if k < 2 else full.at[s, pl.ds((k - 2) * (tokens // 2), tokens // 2)]
        return pltpu.make_async_remote_copy(
            ref, ref, y_out.at[k], y_in.at[k], device_id=device(me, to)
        )

    sends = [pass_on(y, 0, right), pass_on(y, 1, left)]
    for copy in sends:
        copy.start()
    pass_on(left, 0, left).wait_recv()
    sends.append(pass_on(left, 2, right))
    sends[-1].start()
    pass_on(right, 1, right).wait_recv()
    sends.append(pass_on(right, 3, left))
    sends[-1].start()
    pass_on(far, 2, right).wait_recv()
    pass_on(far, 3, left).wait_recv()
    for copy in sends:
        copy.wait_send()


def combine(select, back, cot):
    tokens, width = cot.shape
    dma = pltpu.SemaphoreType.DMA
    return pl.pallas_call(
        combine_kernel,
        out_shape=jax.ShapeDtypeStruct((TP, tokens, width // TP), BF),
        in_specs=[VMEM] * 3,
        out_specs=VMEM,
        scratch_shapes=[dma((4,)), dma((4,))],
        compiler_params=pltpu.CompilerParams(
            collective_id=2, has_side_effects=True, vmem_limit_bytes=40 * 2**20
        ),
        name="combine",
    )(select, back, cot)


def from_behind(x, axis, by):
    devices = lax.axis_size(axis)
    pairs = [(i, i + by) for i in range(devices) if 0 <= i + by < devices]
    return lax.ppermute(x, axis, pairs)


def per_device(
    hidden_in, cotangent, routes, routing_weights, w_gate, w_up, w_down, b_gate, c_gate, x_in, taps, w_out
):
    tokens, width = hidden_in.shape
    share = width // TP
    y = lax.axis_index("tp")
    send, own, select = pack(routes, routing_weights, hidden_in, cotangent)
    got = dispatch(send, own)
    part, d_pre, d_up, hid = experts(got, w_gate[0], w_up[0], w_down[0])
    rows = got.reshape(TP, SP * ROWS, share)
    back = return_rows(part)
    full = combine(select, back, cotangent)
    residual_grad = lax.dynamic_index_in_dim(full, y, 0, keepdims=False)

    def weight_grad(d):
        grad = jnp.einsum("krd,rf->kdf", rows, d, preferred_element_type=F32)
        return grad.astype(BF).reshape(1, width, -1)

    grad_gate, grad_up = weight_grad(d_pre), weight_grad(d_up)
    grad_down = jnp.einsum("rf,krd->fkd", hid, rows, preferred_element_type=F32)
    grad_down = grad_down.astype(BF).reshape(1, -1, width)

    taps_f = taps.astype(F32)
    gated = c_gate.astype(F32) * x_in.astype(F32)
    padded = jnp.concatenate([from_behind(gated[tokens - 2 :], "sp", 1), gated], axis=0)
    conv = (
        taps_f[0] * padded[0:tokens]
        + taps_f[1] * padded[1 : tokens + 1]
        + taps_f[2] * padded[2 : tokens + 2]
    )
    b_f = b_gate.astype(F32)
    y_short = (b_f * conv).astype(BF)
    w_parts = w_out.reshape(TP, share, -1)
    d_y = jnp.einsum("ktd,kdc->tc", full, w_parts, preferred_element_type=F32)
    grad_b = (d_y * conv).astype(BF)
    d_conv = b_f * d_y
    later = jnp.concatenate([d_conv, from_behind(d_conv[0:2], "sp", -1)], axis=0)
    d_v = (
        taps_f[2] * later[0:tokens]
        + taps_f[1] * later[1 : tokens + 1]
        + taps_f[0] * later[2 : tokens + 2]
    )
    grad_c = (d_v * x_in.astype(F32)).astype(BF)
    grad_x = (d_v * c_gate.astype(F32)).astype(BF)
    out_part = jnp.einsum("ktd,tc->kdc", full, y_short, preferred_element_type=F32).astype(BF)
    out_part = out_part.reshape(SP, width // SP, -1)
    arrived = lax.all_to_all(out_part, "sp", split_axis=0, concat_axis=0, tiled=True)
    out_proj_grad = arrived.astype(F32).sum(axis=0)
    return (grad_gate, grad_up, grad_down, out_proj_grad, residual_grad, grad_b, grad_c, grad_x)


def solution(mesh):
    seq, both = P("sp", None), P("sp", "tp")
    return jax.shard_map(
        per_device,
        mesh=mesh,
        in_specs=(
            seq,
            seq,
            seq,
            seq,
            P("sp", None, "tp"),
            P("sp", None, "tp"),
            P("sp", "tp", None),
            both,
            both,
            both,
            P(None, "tp"),
            P(None, "tp"),
        ),
        out_specs=(
            P("sp", None, "tp"),
            P("sp", None, "tp"),
            P("sp", "tp", None),
            both,
            both,
            both,
            both,
            both,
        ),
        check_vma=False,
    )
```

```python
import functools

import jax
import jax.numpy as jnp
from jax import lax
from jax.experimental import pallas as pl
from jax.experimental.pallas import tpu as pltpu
from jax.sharding import PartitionSpec as P

PLANES, PLANE, TP, CAP = 8, 8, 4, 12
SP = PLANES * PLANE
ROWS = 2 * CAP
VMEM = pl.BlockSpec(memory_space=pltpu.VMEM)
BF, F32 = jnp.bfloat16, jnp.float32


def dot(a, b, dims=((1,), (0,))):
    return lax.dot_general(a, b, (dims, ((), ())), preferred_element_type=F32)


def device(sp, tp):
    return {"sp": sp, "tp": tp}


def plane_step(g):
    return ((g + 1) // 2) * (2 * (g % 2) - 1)


def greet_all(me, y, right, left):
    barrier = pltpu.get_barrier_semaphore()

    def signal(i, c):
        pl.semaphore_signal(barrier, inc=1, device_id=device((me + i) % SP, y))
        return c

    lax.fori_loop(1, SP, signal, 0)
    pl.semaphore_signal(barrier, inc=1, device_id=device(me, right))
    pl.semaphore_signal(barrier, inc=1, device_id=device(me, left))
    return barrier


def wait_bytes(ref, sem):
    pltpu.make_async_copy(ref, ref, sem).wait()


def kernel(
    routes, weights, taps, hidden_hbm, cot_hbm, w_gate_hbm, w_up_hbm, w_down_hbm, w_out_hbm, b_hbm, c_hbm, x_hbm,
    grad_gate, grad_up, grad_down, grad_out, residual, grad_b, grad_c, grad_x,
    hidden, cot, w_gate, w_up, w_down, w_out, b_gate, c_gate, x_in,
    send, own, select, got, part, near_in, total_in, sums, back, d_both, hid_rows, full, y_short,
    edge, edge_in, outs, outs_in, plane_sum, plane_in,
    ld, z_in, z_out, f_in, f_out, y_in, y_out, a_in, a_out, b_in, b_out, r_in, r_out,
    h_in, h_out, e_in, e_out, o_in, o_out, q_in, q_out,
):
    me, y = lax.axis_index("sp"), lax.axis_index("tp")
    z, cell = me // PLANE, me % PLANE
    right, left, far = (y + 1) % TP, (y + 3) % TP, (y + 2) % TP
    tokens, width = hidden.shape
    share = width // TP
    half_share = share // 2
    part_rows = PLANE * ROWS
    slots = SP * ROWS
    mid = PLANE // 2
    ff = w_gate.shape[1]

    loads = [
        pltpu.make_async_copy(a, b, ld.at[i])
        for i, (a, b) in enumerate(
            (
                (hidden_hbm, hidden),
                (cot_hbm, cot),
                (c_hbm, c_gate),
                (x_hbm, x_in),
                (w_gate_hbm, w_gate),
                (w_up_hbm, w_up),
                (w_down_hbm, w_down),
                (b_hbm, b_gate),
                (w_out_hbm, w_out),
            )
        )
    ]
    for load in loads:
        load.start()
    barrier = greet_all(me, y, right, left)

    down = lax.broadcasted_iota(jnp.int32, (tokens, tokens), 0)
    across = lax.broadcasted_iota(jnp.int32, (tokens, tokens), 1)

    def count(match):
        return jnp.sum(jnp.where(match, 1.0, 0.0), axis=0, keepdims=True).astype(jnp.int32)

    r0, r1 = routes[0:1, :], routes[1:2, :]
    w0, w1 = weights[0:1, :], weights[1:2, :]
    c0 = jnp.sum(jnp.where(down == across, r0, 0), axis=1, keepdims=True)
    c1 = jnp.sum(jnp.where(down == across, r1, 0), axis=1, keepdims=True)
    earlier = down < across
    t0 = r0 * ROWS + count(earlier & (c0 == r0))
    t1 = r1 * ROWS + count(c0 == r1) + count(earlier & (c1 == r1))
    row = lax.broadcasted_iota(jnp.int32, (part_rows, tokens), 0)
    is_token = lax.broadcasted_iota(jnp.int32, (part_rows, 1), 0) % ROWS < CAP

    def picks(plane):
        slot = row + plane * part_rows
        h = jnp.where((t0 == slot) | (t1 == slot), 1.0, 0.0)
        s0, s1 = t0 + CAP == slot, t1 + CAP == slot
        s = jnp.where(s0 | s1, 1.0, 0.0)
        scale = jnp.sum(jnp.where(s0, w0, 0.0) + jnp.where(s1, w1, 0.0), axis=1, keepdims=True)
        select[pl.ds(pl.multiple_of(plane * part_rows, part_rows), part_rows), :] = (h + s).astype(BF)
        return h.astype(BF), s.astype(BF), jnp.where(is_token, 1.0, scale)

    def plane_of(g, sign):
        return (z + sign * plane_step(g) + PLANES) % PLANES

    mine = pl.ds(pl.multiple_of(y * share, share), share)

    def pack(g):
        plane = plane_of(g, 1)
        h, s, scale = picks(plane)
        rows = (dot(h, hidden[:, mine]) + dot(s, cot[:, mine])) * scale
        send[pl.ds(plane * PLANE, PLANE)] = rows.astype(BF).reshape(PLANE, ROWS, share)

    def send_group(g):
        def one(j, c):
            to = plane_of(g, 1) * PLANE + (cell + j) % PLANE
            pltpu.make_async_remote_copy(
                send.at[to], got.at[y, me], z_out, z_in.at[g], device_id=device(to, y)
            ).start()
            return c

        lax.fori_loop(0, PLANE, one, 0)

    loads[0].wait()
    loads[1].wait()
    pack(1)
    pl.semaphore_wait(barrier, SP + 1)

    def pack_ahead(g, c):
        pack(g + 1)
        send_group(g)
        return c

    lax.fori_loop(1, 3, pack_ahead, 0)
    h, s, scale = picks(z)
    for k in range(TP):
        cols = pl.ds(k * share, share)
        rows = (dot(h, hidden[:, cols]) + dot(s, cot[:, cols])) * scale
        own[k] = rows.astype(BF).reshape(PLANE, ROWS, share)
    send_group(3)
    for k in range(TP):
        got[k, me] = own[k, cell]

    def send_full(i, c):
        j, k = (cell + 1 + i % (PLANE - 1)) % PLANE, i // (PLANE - 1)
        pltpu.make_async_remote_copy(
            own.at[k, j], got.at[k, me], f_out, f_in, device_id=device(z * PLANE + j, y)
        ).start()
        return c

    near = TP * (PLANE - 1)
    lax.fori_loop(0, near, send_full, 0)
    pack(4)
    lax.fori_loop(4, PLANES - 1, pack_ahead, 0)

    loads[2].wait()
    loads[3].wait()
    edge[0] = c_gate[tokens - 8 :, :].astype(F32) * x_in[tokens - 8 :, :].astype(F32)
    send_group(PLANES - 1)

    def edge_copy(k, by):
        return pltpu.make_async_remote_copy(
            edge.at[k], edge_in.at[k], h_out.at[k], h_in.at[k], device_id=device((me + by + SP) % SP, y)
        )

    edge_copy(0, 1).start()
    for load in loads[4:7]:
        load.wait()

    def block(k, g, at=0, size=PLANE):
        return got.at[k, pl.ds(plane_of(g, -1) * PLANE + at, size)]

    def pass_on(s, g, k, to):
        ref = block(s, g) if k < 2 else block(s, g, (k - 2) * mid, mid)
        return pltpu.make_async_remote_copy(
            ref, ref, y_out.at[k], y_in.at[k, g], device_id=device(me, to)
        )

    def expert_rows(g):
        plane = plane_of(g, -1)
        blocks = pl.ds(plane * PLANE, PLANE)
        pre_gate = pre_up = d_hid = jnp.zeros((part_rows, ff), F32)
        for k in range(TP):
            x = got[k, blocks].reshape(part_rows, share)
            cols = pl.ds(k * share, share)
            pre_gate += dot(x, w_gate[cols, :])
            pre_up += dot(x, w_up[cols, :])
            d_hid += dot(x, w_down[:, cols], ((1,), (1,)))
        d_hid = pltpu.roll(d_hid, part_rows - CAP, 0)
        sigma = 1.0 / (1.0 + jnp.exp(-pre_gate))
        silu = pre_gate * sigma
        d_up = d_hid * silu
        d_pre = d_hid * pre_up * sigma * (1.0 + pre_gate * (1.0 - sigma))
        twice_pre = jnp.where(is_token, d_pre, pltpu.roll(d_pre, CAP, 0)).astype(BF)
        twice_up = jnp.where(is_token, d_up, pltpu.roll(d_up, CAP, 0)).astype(BF)
        for k in range(TP):
            cols = pl.ds(k * share, share)
            grad = dot(twice_pre, w_gate[cols, :], ((1,), (1,)))
            grad += dot(twice_up, w_up[cols, :], ((1,), (1,)))
            folded = jnp.where(is_token, grad[:, :half_share], grad[:, half_share:])
            part[k, blocks] = folded.astype(BF).reshape(PLANE, ROWS, half_share)
        at = pl.ds(pl.multiple_of(plane * part_rows, part_rows), part_rows)
        d_both[at, 0:ff] = jnp.where(is_token, d_pre, 0.0).astype(BF)
        d_both[at, ff:] = jnp.where(is_token, d_up, 0.0).astype(BF)
        hid_rows[at, :] = jnp.where(is_token, 0.0, pltpu.roll(silu * pre_up, CAP, 0)).astype(BF)

    def far_half(g, k, to):
        at = plane_of(g, -1) * PLANE + k * mid
        return pltpu.make_async_remote_copy(
            part.at[far, pl.ds(at, mid)], near_in.at[k, g], a_out.at[k], a_in.at[k, g],
            device_id=device(me, to),
        )

    def near_sum(g, k, to):
        return pltpu.make_async_remote_copy(
            part.at[to, pl.ds(plane_of(g, -1) * PLANE, PLANE)], total_in.at[k, g], b_out.at[k],
            b_in.at[k, g], device_id=device(me, to),
        )

    def add(g, k, to):
        at = pl.ds(plane_of(g, -1) * PLANE + k * mid, mid)
        part[to, at] = (part[to, at].astype(F32) + near_in[k, g].astype(F32)).astype(BF)

    def send_back(g, j):
        to = plane_of(g, -1) * PLANE + (cell + j) % PLANE
        pltpu.make_async_remote_copy(
            sums.at[to], back.at[me], r_out, r_in, device_id=device(to, y)
        ).start()

    def step(t, c):
        @pl.when(t < PLANES)
        def _():
            wait_bytes(block(y, t), z_in.at[t])
            pass_on(y, t, 0, right).start()
            pass_on(y, t, 1, left).start()

        @pl.when((t > 1) & (t <= PLANES))
        def _():
            g = t - 1
            pass_on(left, g, 0, left).wait_recv()
            pass_on(left, g, 2, right).start()
            pass_on(right, g, 1, right).wait_recv()
            pass_on(right, g, 3, left).start()

        @pl.when((t >= 4) & (t < PLANES + 4))
        def _():
            g = t - 4
            far_half(g, 0, right).wait_recv()
            add(g, 0, right)
            far_half(g, 1, left).wait_recv()
            add(g, 1, left)

        @pl.when(t >= 5)
        def _():
            g = t - 5
            near_sum(g, 0, right).wait_recv()
            near_sum(g, 1, left).wait_recv()
            at = pl.ds(plane_of(g, -1) * PLANE, PLANE)
            sums[at] = (
                part[y, at].astype(F32) + total_in[0, g].astype(F32) + total_in[1, g].astype(F32)
            ).astype(BF)

        @pl.when((t >= 4) & (t < PLANES + 4))
        def _():
            near_sum(t - 4, 0, right).start()
            near_sum(t - 4, 1, left).start()

        @pl.when(t >= 5)
        def _():
            g = t - 5

            @pl.when(g > 0)
            def _():
                send_back(g, 0)

            lax.fori_loop(1, PLANE, lambda j, d: (send_back(g, j), d)[1], 0)

        @pl.when(t == 2)
        def _():
            wait_bytes(got.at[0, pl.ds(0, near)], f_in)

        @pl.when((t > 2) & (t < PLANES + 2))
        def _():
            pass_on(far, t - 2, 2, right).wait_recv()
            pass_on(far, t - 2, 3, left).wait_recv()

        @pl.when((t >= 2) & (t < PLANES + 2))
        def _():
            expert_rows(t - 2)
            far_half(t - 2, 0, right).start()
            far_half(t - 2, 1, left).start()

        return c

    lax.fori_loop(1, PLANES + 5, step, 0)
    back[me] = sums[me]

    wait_bytes(part.at[0, pl.ds(0, SP - 1)], r_in)
    token_slot = lax.broadcasted_iota(jnp.int32, (slots, 1), 0) % ROWS < CAP
    rows = back[...].reshape(slots, half_share)
    zero = jnp.zeros_like(rows)
    kept = jnp.concatenate(
        [jnp.where(token_slot, rows, zero), jnp.where(token_slot, zero, rows)], axis=1
    )
    total = (cot[:, mine].astype(F32) + dot(select[...], kept, ((0,), (0,)))).astype(BF)
    full[y] = total
    residual[...] = total

    def spread(s, k, to):
        ref = full.at[s] if k < 2 else full.at[s, pl.ds((k - 2) * (tokens // 2), tokens // 2)]
        return pltpu.make_async_remote_copy(
            ref, ref, e_out.at[k], e_in.at[k], device_id=device(me, to)
        )

    def weight_grads(k, c):
        rows = got[k].reshape(slots, share)
        at = pl.ds(pl.multiple_of(k * share, share), share)
        both = dot(rows, d_both[...], ((0,), (0,)))
        grad_gate[at, :] = both[:, :ff].astype(BF)
        grad_up[at, :] = both[:, ff:].astype(BF)
        grad_down[:, at] = dot(hid_rows[...], rows, ((0,), (0,))).astype(BF)
        return c

    sends = [spread(y, 0, right), spread(y, 1, left)]
    for copy in sends:
        copy.start()
    t_row = lax.broadcasted_iota(jnp.int32, (tokens, 1), 0)
    tap = [taps[i : i + 1, :].astype(F32) for i in range(3)]
    gated = c_gate[...].astype(F32) * x_in[...].astype(F32)
    edge_copy(0, 1).wait_recv()
    before = jnp.where(me == 0, 0.0, edge_in[0])
    one_back = jnp.where(t_row == 0, before[7:8], pltpu.roll(gated, 1, 0))
    two_back = jnp.where(
        t_row == 0, before[6:7], jnp.where(t_row == 1, before[7:8], pltpu.roll(gated, 2, 0))
    )
    conv = tap[0] * two_back + tap[1] * one_back + tap[2] * gated
    loads[7].wait()
    b_f = b_gate[...].astype(F32)
    y_short[...] = (b_f * conv).astype(BF)
    loads[8].wait()
    spread(left, 0, left).wait_recv()
    sends.append(spread(left, 2, right))
    sends[-1].start()
    spread(right, 1, right).wait_recv()
    sends.append(spread(right, 3, left))
    sends[-1].start()
    lax.fori_loop(0, 2, weight_grads, 0)
    spread(far, 2, right).wait_recv()
    spread(far, 3, left).wait_recv()

    for k in range(TP):
        grad = dot(full[k], y_short[...], ((0,), (0,))).astype(BF)
        for zz in range(2):
            for j in range(PLANE):
                at = (zz * PLANE + j) * 32
                outs[j, 2 * k + zz] = grad[at : at + 32]

    d_y = jnp.zeros((tokens, w_out.shape[1]), F32)
    for k in range(TP):
        d_y += dot(full[k], w_out[pl.ds(k * share, share), :])

    def send_out(j, c):
        to = (cell + j) % PLANE
        pltpu.make_async_remote_copy(
            outs.at[to], outs_in.at[cell], o_out, o_in, device_id=device(z * PLANE + to, y)
        ).start()
        return c

    lax.fori_loop(1, PLANE, send_out, 0)
    d_conv = b_f * d_y
    edge[1] = d_conv[0:8]
    grad_b[...] = (d_y * conv).astype(BF)
    edge_copy(1, -1).start()
    lax.fori_loop(2, 3, weight_grads, 0)
    edge_copy(1, -1).wait_recv()
    after = jnp.where(me == SP - 1, 0.0, edge_in[1])
    one_on = jnp.where(t_row == tokens - 1, after[0:1], pltpu.roll(d_conv, tokens - 1, 0))
    two_on = jnp.where(
        t_row == tokens - 2,
        after[0:1],
        jnp.where(t_row == tokens - 1, after[1:2], pltpu.roll(d_conv, tokens - 2, 0)),
    )
    d_v = tap[2] * d_conv + tap[1] * one_on + tap[0] * two_on
    grad_c[...] = (d_v * x_in[...].astype(F32)).astype(BF)
    grad_x[...] = (d_v * c_gate[...].astype(F32)).astype(BF)
    wait_bytes(outs_in.at[pl.ds(0, PLANE - 1)], o_in)

    def sum_plane(p, c):
        acc = outs[cell, p].astype(F32)
        for j in range(1, PLANE):
            acc += outs_in[(cell + j) % PLANE, p].astype(F32)
        plane_sum[p] = acc.astype(BF)
        return c

    lax.fori_loop(0, PLANES, sum_plane, 0)

    def send_sum(i, c):
        to = (z + i) % PLANES
        pltpu.make_async_remote_copy(
            plane_sum.at[to], plane_in.at[z], q_out, q_in, device_id=device(to * PLANE + cell, y)
        ).start()
        return c

    lax.fori_loop(1, PLANES, send_sum, 0)
    lax.fori_loop(3, 4, weight_grads, 0)
    wait_bytes(plane_in.at[pl.ds(0, PLANES - 1)], q_in)
    acc = plane_sum[z].astype(F32)
    for i in range(1, PLANES):
        acc += plane_in[(z + i) % PLANES].astype(F32)
    grad_out[...] = acc

    wait_bytes(got.at[0, pl.ds(0, SP - PLANE)], z_out)
    wait_bytes(got.at[0, pl.ds(0, near)], f_out)
    for k in range(4):
        size = PLANE if k < 2 else mid
        wait_bytes(got.at[0, pl.ds(0, size * (PLANES - 1))], y_out.at[k])
    for k in range(2):
        wait_bytes(part.at[0, pl.ds(0, SP // 2)], a_out.at[k])
        wait_bytes(part.at[0], b_out.at[k])
        edge_copy(k, 1).wait_send()
    wait_bytes(part.at[0, pl.ds(0, SP - 1)], r_out)
    for copy in sends:
        copy.wait_send()
    wait_bytes(outs_in.at[pl.ds(0, PLANE - 1)], o_out)
    wait_bytes(plane_in.at[pl.ds(0, PLANES - 1)], q_out)


def per_device(
    hidden_in, cotangent, routes, routing_weights, w_gate, w_up, w_down, b_gate, c_gate, x_in, taps, w_out
):
    tokens, width = hidden_in.shape
    share, ff, short = width // TP, w_gate.shape[2], x_in.shape[1]
    half = share // 2
    slots, out_rows = SP * ROWS, width // SP
    like, dma = jax.ShapeDtypeStruct, pltpu.SemaphoreType.DMA
    hbm = pl.BlockSpec(memory_space=pl.ANY)
    outs = pl.pallas_call(
        kernel,
        out_shape=(
            like((width, ff), BF),
            like((width, ff), BF),
            like((ff, width), BF),
            like((out_rows, short), F32),
            like((tokens, share), BF),
            like((tokens, short), BF),
            like((tokens, short), BF),
            like((tokens, short), BF),
        ),
        in_specs=[VMEM] * 3 + [hbm] * 9,
        out_specs=(VMEM,) * 8,
        scratch_shapes=[
            pltpu.VMEM((tokens, width), BF),
            pltpu.VMEM((tokens, width), BF),
            pltpu.VMEM((width, ff), BF),
            pltpu.VMEM((width, ff), BF),
            pltpu.VMEM((ff, width), BF),
            pltpu.VMEM((width, short), BF),
            pltpu.VMEM((tokens, short), BF),
            pltpu.VMEM((tokens, short), BF),
            pltpu.VMEM((tokens, short), BF),
            pltpu.VMEM((SP, ROWS, share), BF),
            pltpu.VMEM((TP, PLANE, ROWS, share), BF),
            pltpu.VMEM((slots, tokens), BF),
            pltpu.VMEM((TP, SP, ROWS, share), BF),
            pltpu.VMEM((TP, SP, ROWS, half), BF),
            pltpu.VMEM((2, PLANES, PLANE // 2, ROWS, half), BF),
            pltpu.VMEM((2, PLANES, PLANE, ROWS, half), BF),
            pltpu.VMEM((SP, ROWS, half), BF),
            pltpu.VMEM((SP, ROWS, half), BF),
            pltpu.VMEM((slots, 2 * ff), BF),
            pltpu.VMEM((slots, ff), BF),
            pltpu.VMEM((TP, tokens, share), BF),
            pltpu.VMEM((tokens, short), BF),
            pltpu.VMEM((2, 8, short), F32),
            pltpu.VMEM((2, 8, short), F32),
            pltpu.VMEM((PLANE, PLANES, out_rows, short), BF),
            pltpu.VMEM((PLANE, PLANES, out_rows, short), BF),
            pltpu.VMEM((PLANES, out_rows, short), BF),
            pltpu.VMEM((PLANES, out_rows, short), BF),
            dma((9,)),
            dma((PLANES,)),
            dma(()),
            dma(()),
            dma(()),
            dma((4, PLANES)),
            dma((4,)),
            dma((2, PLANES)),
            dma((2,)),
            dma((2, PLANES)),
            dma((2,)),
            dma(()),
            dma(()),
            dma((2,)),
            dma((2,)),
            dma((4,)),
            dma((4,)),
            dma(()),
            dma(()),
            dma(()),
            dma(()),
        ],
        compiler_params=pltpu.CompilerParams(
            collective_id=0, has_side_effects=True, vmem_limit_bytes=62 * 2**20
        ),
        name="layer",
    )(
        routes.T, routing_weights.T, taps, hidden_in, cotangent, w_gate[0], w_up[0], w_down[0], w_out,
        b_gate, c_gate, x_in,
    )
    grad_gate, grad_up, grad_down, grad_out, residual, grad_b, grad_c, grad_x = outs
    return grad_gate[None], grad_up[None], grad_down[None], grad_out, residual, grad_b, grad_c, grad_x


def solution(mesh):
    seq, both = P("sp", None), P("sp", "tp")
    return jax.shard_map(
        per_device,
        mesh=mesh,
        in_specs=(
            seq,
            seq,
            seq,
            seq,
            P("sp", None, "tp"),
            P("sp", None, "tp"),
            P("sp", "tp", None),
            both,
            both,
            both,
            P(None, "tp"),
            P(None, "tp"),
        ),
        out_specs=(
            P("sp", None, "tp"),
            P("sp", None, "tp"),
            P("sp", "tp", None),
            both,
            both,
            both,
            both,
            both,
        ),
        check_vma=False,
    )
```

```python
import functools

import jax
import jax.numpy as jnp
from jax import lax
from jax.experimental import pallas as pl
from jax.experimental.pallas import tpu as pltpu
from jax.sharding import PartitionSpec as P

PLANES, PLANE, TP, CAP = 8, 8, 4, 12
SP = PLANES * PLANE
ROWS = 2 * CAP
VMEM = pl.BlockSpec(memory_space=pltpu.VMEM)
BF, F32 = jnp.bfloat16, jnp.float32


def dot(a, b, dims=((1,), (0,))):
    return lax.dot_general(a, b, (dims, ((), ())), preferred_element_type=F32)


def device(sp, tp):
    return {"sp": sp, "tp": tp}


STEPS = (0, 2, 6, 3, 5, 4, 1, 7)
NEAR = (0, 6, 7)
FAR = range(1, 6)
NEAR_AT = 3


def plane_step(g):
    if isinstance(g, int):
        return STEPS[g]
    return sum(jnp.where(g == i, step, 0) for i, step in enumerate(STEPS))


def greet_all(me, y, right, left):
    barrier = pltpu.get_barrier_semaphore()

    def signal(i, c):
        pl.semaphore_signal(barrier, inc=1, device_id=device((me + i) % SP, y))
        return c

    lax.fori_loop(1, SP, signal, 0)
    pl.semaphore_signal(barrier, inc=1, device_id=device(me, right))
    pl.semaphore_signal(barrier, inc=1, device_id=device(me, left))
    return barrier


def wait_bytes(ref, sem):
    pltpu.make_async_copy(ref, ref, sem).wait()


def kernel(
    routes, weights, taps, hidden_hbm, cot_hbm, w_gate_hbm, w_up_hbm, w_down_hbm, w_out_hbm, b_hbm, c_hbm, x_hbm,
    grad_gate, grad_up, grad_down, grad_out, residual, grad_b, grad_c, grad_x,
    hidden, cot, w_gate, w_up, w_down, w_out, b_gate, c_gate, x_in,
    send, own, select, got, part, near_in, total_in, sums, back, d_both, hid_rows, full, y_short,
    edge, edge_in, outs, outs_in, plane_sum, plane_in,
    ld, z_in, z_out, f_in, f_out, y_in, y_out, a_in, a_out, b_in, b_out, r_in, r_out,
    h_in, h_out, e_in, e_out, o_in, o_out, q_in, q_out,
):
    me, y = lax.axis_index("sp"), lax.axis_index("tp")
    z, cell = me // PLANE, me % PLANE
    right, left, far = (y + 1) % TP, (y + 3) % TP, (y + 2) % TP
    tokens, width = hidden.shape
    share = width // TP
    half_share = share // 2
    part_rows = PLANE * ROWS
    slots = SP * ROWS
    mid = PLANE // 2
    ff = w_gate.shape[1]
    out_rows = grad_out.shape[0]

    loads = [
        pltpu.make_async_copy(a, b, ld.at[i])
        for i, (a, b) in enumerate(
            (
                (hidden_hbm, hidden),
                (cot_hbm, cot),
                (c_hbm, c_gate),
                (x_hbm, x_in),
                (w_gate_hbm, w_gate),
                (w_up_hbm, w_up),
                (w_down_hbm, w_down),
                (b_hbm, b_gate),
                (w_out_hbm, w_out),
            )
        )
    ]
    for load in loads:
        load.start()
    barrier = greet_all(me, y, right, left)

    down = lax.broadcasted_iota(jnp.int32, (tokens, tokens), 0)
    across = lax.broadcasted_iota(jnp.int32, (tokens, tokens), 1)

    def count(match):
        return jnp.sum(jnp.where(match, 1.0, 0.0), axis=0, keepdims=True).astype(jnp.int32)

    r0, r1 = routes[0:1, :], routes[1:2, :]
    w0, w1 = weights[0:1, :], weights[1:2, :]
    c0 = jnp.sum(jnp.where(down == across, r0, 0), axis=1, keepdims=True)
    c1 = jnp.sum(jnp.where(down == across, r1, 0), axis=1, keepdims=True)
    earlier = down < across
    t0 = r0 * ROWS + count(earlier & (c0 == r0))
    t1 = r1 * ROWS + count(c0 == r1) + count(earlier & (c1 == r1))
    row = lax.broadcasted_iota(jnp.int32, (part_rows, tokens), 0)
    is_token = lax.broadcasted_iota(jnp.int32, (part_rows, 1), 0) % ROWS < CAP

    def picks(plane):
        slot = row + plane * part_rows
        h = jnp.where((t0 == slot) | (t1 == slot), 1.0, 0.0)
        s0, s1 = t0 + CAP == slot, t1 + CAP == slot
        s = jnp.where(s0 | s1, 1.0, 0.0)
        scale = jnp.sum(jnp.where(s0, w0, 0.0) + jnp.where(s1, w1, 0.0), axis=1, keepdims=True)
        select[pl.ds(pl.multiple_of(plane * part_rows, part_rows), part_rows), :] = (h + s).astype(BF)
        return h.astype(BF), s.astype(BF), jnp.where(is_token, 1.0, scale)

    def plane_of(g, sign):
        return (z + sign * plane_step(g) + PLANES) % PLANES

    mine = pl.ds(pl.multiple_of(y * share, share), share)

    def pack(g):
        plane = plane_of(g, 1)
        h, s, scale = picks(plane)
        rows = (dot(h, hidden[:, mine]) + dot(s, cot[:, mine])) * scale
        send[pl.ds(plane * PLANE, PLANE)] = rows.astype(BF).reshape(PLANE, ROWS, share)

    def send_group(g):
        def one(j, c):
            to = plane_of(g, 1) * PLANE + (cell + j) % PLANE
            pltpu.make_async_remote_copy(
                send.at[to], got.at[y, me], z_out, z_in.at[g], device_id=device(to, y)
            ).start()
            return c

        lax.fori_loop(0, PLANE, one, 0)

    loads[0].wait()
    loads[1].wait()
    def pack_full(n):
        plane = plane_of(NEAR[n], 1)
        h, s, scale = picks(plane)
        for k in range(TP):
            cols = pl.ds(k * share, share)
            rows = (dot(h, hidden[:, cols]) + dot(s, cot[:, cols])) * scale
            own[n, k] = rows.astype(BF).reshape(PLANE, ROWS, share)

    def send_full(n, first):
        count = PLANE - first

        def one(i, c):
            j, k = (cell + first + i % count) % PLANE, i // count
            to = plane_of(NEAR[n], 1) * PLANE + j
            pltpu.make_async_remote_copy(
                own.at[n, k, j], got.at[k, me], f_out.at[n], f_in.at[n], device_id=device(to, y)
            ).start()
            return c

        lax.fori_loop(0, TP * count, one, 0)

    lax.fori_loop(FAR[0], FAR[-1] + 1, lambda g, c: (pack(g), c)[1], 0)
    pack_full(0)
    for k in range(TP):
        got[k, me] = own[0, k, cell]
    pl.semaphore_wait(barrier, SP + 1)
    lax.fori_loop(1, 3, lambda g, c: (send_group(g), c)[1], 0)
    send_full(0, 1)
    lax.fori_loop(3, FAR[-1] + 1, lambda g, c: (send_group(g), c)[1], 0)
    pack_full(1)
    pack_full(2)

    loads[2].wait()
    loads[3].wait()
    edge[0] = c_gate[tokens - 8 :, :].astype(F32) * x_in[tokens - 8 :, :].astype(F32)

    def edge_copy(k, by):
        return pltpu.make_async_remote_copy(
            edge.at[k], edge_in.at[k], h_out.at[k], h_in.at[k], device_id=device((me + by + SP) % SP, y)
        )

    edge_copy(0, 1).start()
    for load in loads[4:7]:
        load.wait()

    def block(k, g, at=0, size=PLANE):
        return got.at[k, pl.ds(plane_of(g, -1) * PLANE + at, size)]

    def pass_on(s, g, k, to):
        ref = block(s, g) if k < 2 else block(s, g, (k - 2) * mid, mid)
        return pltpu.make_async_remote_copy(
            ref, ref, y_out.at[k], y_in.at[k, g], device_id=device(me, to)
        )

    def expert_rows(g):
        plane = plane_of(g, -1)
        blocks = pl.ds(plane * PLANE, PLANE)
        pre_gate = pre_up = d_hid = jnp.zeros((part_rows, ff), F32)
        for k in range(TP):
            x = got[k, blocks].reshape(part_rows, share)
            cols = pl.ds(k * share, share)
            pre_gate += dot(x, w_gate[cols, :])
            pre_up += dot(x, w_up[cols, :])
            d_hid += dot(x, w_down[:, cols], ((1,), (1,)))
        d_hid = pltpu.roll(d_hid, part_rows - CAP, 0)
        sigma = 1.0 / (1.0 + jnp.exp(-pre_gate))
        silu = pre_gate * sigma
        d_up = d_hid * silu
        d_pre = d_hid * pre_up * sigma * (1.0 + pre_gate * (1.0 - sigma))
        twice_pre = jnp.where(is_token, d_pre, pltpu.roll(d_pre, CAP, 0)).astype(BF)
        twice_up = jnp.where(is_token, d_up, pltpu.roll(d_up, CAP, 0)).astype(BF)
        for k in range(TP):
            cols = pl.ds(k * share, share)
            grad = dot(twice_pre, w_gate[cols, :], ((1,), (1,)))
            grad += dot(twice_up, w_up[cols, :], ((1,), (1,)))
            folded = jnp.where(is_token, grad[:, :half_share], grad[:, half_share:])
            part[k, blocks] = folded.astype(BF).reshape(PLANE, ROWS, half_share)
        at = pl.ds(pl.multiple_of(plane * part_rows, part_rows), part_rows)
        d_both[at, 0:ff] = jnp.where(is_token, d_pre, 0.0).astype(BF)
        d_both[at, ff:] = jnp.where(is_token, d_up, 0.0).astype(BF)
        hid_rows[at, :] = jnp.where(is_token, 0.0, pltpu.roll(silu * pre_up, CAP, 0)).astype(BF)

    def far_half(g, k, to):
        at = plane_of(g, -1) * PLANE + k * mid
        return pltpu.make_async_remote_copy(
            part.at[far, pl.ds(at, mid)], near_in.at[k, g], a_out.at[k], a_in.at[k, g],
            device_id=device(me, to),
        )

    def near_sum(g, k, to):
        return pltpu.make_async_remote_copy(
            part.at[to, pl.ds(plane_of(g, -1) * PLANE, PLANE)], total_in.at[k, g], b_out.at[k],
            b_in.at[k, g], device_id=device(me, to),
        )

    def add(g, k, to):
        at = pl.ds(plane_of(g, -1) * PLANE + k * mid, mid)
        part[to, at] = (part[to, at].astype(F32) + near_in[k, g].astype(F32)).astype(BF)

    def send_back(g, j):
        to = plane_of(g, -1) * PLANE + (cell + j) % PLANE
        pltpu.make_async_remote_copy(
            sums.at[to], back.at[me], r_out, r_in, device_id=device(to, y)
        ).start()

    def full_blocks(n):
        return got.at[0, pl.ds(0, TP * (PLANE - 1 if n == 0 else PLANE))]

    def step(t, c):
        @pl.when(t == NEAR_AT)
        def _():
            send_full(1, 0)
            send_full(2, 0)

        @pl.when(t <= FAR[-1])
        def _():
            wait_bytes(block(y, t), z_in.at[t])
            pass_on(y, t, 0, right).start()
            pass_on(y, t, 1, left).start()

        @pl.when((t > 1) & (t <= FAR[-1] + 1))
        def _():
            g = t - 1
            pass_on(left, g, 0, left).wait_recv()
            pass_on(left, g, 2, right).start()
            pass_on(right, g, 1, right).wait_recv()
            pass_on(right, g, 3, left).start()

        @pl.when((t >= 4) & (t < PLANES + 4))
        def _():
            g = t - 4
            far_half(g, 0, right).wait_recv()
            add(g, 0, right)
            far_half(g, 1, left).wait_recv()
            add(g, 1, left)

        @pl.when(t >= 6)
        def _():
            g = t - 6

            @pl.when(g > 0)
            def _():
                send_back(g, 0)

            lax.fori_loop(1, PLANE, lambda j, d: (send_back(g, j), d)[1], 0)

        @pl.when((t >= 4) & (t < PLANES + 4))
        def _():
            near_sum(t - 4, 0, right).start()
            near_sum(t - 4, 1, left).start()

        @pl.when((t >= 5) & (t < PLANES + 5))
        def _():
            g = t - 5
            near_sum(g, 0, right).wait_recv()
            near_sum(g, 1, left).wait_recv()
            at = pl.ds(plane_of(g, -1) * PLANE, PLANE)
            sums[at] = (
                part[y, at].astype(F32) + total_in[0, g].astype(F32) + total_in[1, g].astype(F32)
            ).astype(BF)

        for n, g in enumerate(NEAR):

            @pl.when(t == g + 2)
            def _():
                wait_bytes(full_blocks(n), f_in.at[n])

        @pl.when((t > 2) & (t <= FAR[-1] + 2))
        def _():
            pass_on(far, t - 2, 2, right).wait_recv()
            pass_on(far, t - 2, 3, left).wait_recv()

        @pl.when((t >= 2) & (t < PLANES + 2))
        def _():
            expert_rows(t - 2)
            far_half(t - 2, 0, right).start()
            far_half(t - 2, 1, left).start()

        return c

    lax.fori_loop(1, PLANES + 6, step, 0)
    back[me] = sums[me]

    wait_bytes(part.at[0, pl.ds(0, SP - 1)], r_in)
    token_slot = lax.broadcasted_iota(jnp.int32, (slots, 1), 0) % ROWS < CAP
    rows = back[...].reshape(slots, half_share)
    zero = jnp.zeros_like(rows)
    kept = jnp.concatenate(
        [jnp.where(token_slot, rows, zero), jnp.where(token_slot, zero, rows)], axis=1
    )
    total = (cot[:, mine].astype(F32) + dot(select[...], kept, ((0,), (0,)))).astype(BF)
    full[y] = total
    residual[...] = total

    rows_half = tokens // 2

    def spread(s, at, k, to):
        ref = full.at[s, pl.ds(at * rows_half, rows_half)]
        return pltpu.make_async_remote_copy(
            ref, ref, e_out.at[k], e_in.at[k], device_id=device(me, to)
        )

    def weight_grads(k, c):
        rows = got[k].reshape(slots, share)
        at = pl.ds(pl.multiple_of(k * share, share), share)
        both = dot(rows, d_both[...], ((0,), (0,)))
        grad_gate[at, :] = both[:, :ff].astype(BF)
        grad_up[at, :] = both[:, ff:].astype(BF)
        grad_down[:, at] = dot(hid_rows[...], rows, ((0,), (0,))).astype(BF)
        return c

    sends = [spread(y, 0, 0, right), spread(y, 1, 1, left), spread(y, 1, 2, right), spread(y, 0, 3, left)]
    for copy in sends:
        copy.start()
    t_row = lax.broadcasted_iota(jnp.int32, (tokens, 1), 0)
    tap = [taps[i : i + 1, :].astype(F32) for i in range(3)]
    gated = c_gate[...].astype(F32) * x_in[...].astype(F32)
    edge_copy(0, 1).wait_recv()
    before = jnp.where(me == 0, 0.0, edge_in[0])
    one_back = jnp.where(t_row == 0, before[7:8], pltpu.roll(gated, 1, 0))
    two_back = jnp.where(
        t_row == 0, before[6:7], jnp.where(t_row == 1, before[7:8], pltpu.roll(gated, 2, 0))
    )
    conv = tap[0] * two_back + tap[1] * one_back + tap[2] * gated
    loads[7].wait()
    b_f = b_gate[...].astype(F32)
    y_short[...] = (b_f * conv).astype(BF)
    loads[8].wait()

    def project(k):
        grad = dot(full[k], y_short[...], ((0,), (0,))).astype(BF)
        for zz in range(2):
            for j in range(PLANE):
                at = (zz * PLANE + j) * out_rows
                outs[j, 2 * k + zz] = grad[at : at + out_rows]
        return dot(full[k], w_out[pl.ds(pl.multiple_of(k * share, share), share), :])

    def send_out(k):
        def one(j, c):
            to = (cell + j) % PLANE
            pltpu.make_async_remote_copy(
                outs.at[to, pl.ds(2 * k, 2)],
                outs_in.at[cell, pl.ds(2 * k, 2)],
                o_out,
                o_in,
                device_id=device(z * PLANE + to, y),
            ).start()
            return c

        lax.fori_loop(1, PLANE, one, 0)

    d_y = project(y)
    send_out(y)
    lax.fori_loop(0, 1, weight_grads, 0)
    spread(left, 0, 0, left).wait_recv()
    sends.append(spread(left, 0, 4, right))
    sends[-1].start()
    spread(right, 1, 1, right).wait_recv()
    sends.append(spread(right, 1, 5, left))
    sends[-1].start()
    spread(left, 1, 2, left).wait_recv()
    d_y += project(left)
    send_out(left)
    spread(right, 0, 3, right).wait_recv()
    d_y += project(right)
    send_out(right)
    lax.fori_loop(1, 2, weight_grads, 0)
    spread(far, 0, 4, right).wait_recv()
    spread(far, 1, 5, left).wait_recv()
    d_y += project(far)
    d_conv = b_f * d_y
    edge[1] = d_conv[0:8]
    grad_b[...] = (d_y * conv).astype(BF)
    edge_copy(1, -1).start()
    send_out(far)
    lax.fori_loop(2, 3, weight_grads, 0)
    edge_copy(1, -1).wait_recv()
    after = jnp.where(me == SP - 1, 0.0, edge_in[1])
    one_on = jnp.where(t_row == tokens - 1, after[0:1], pltpu.roll(d_conv, tokens - 1, 0))
    two_on = jnp.where(
        t_row == tokens - 2,
        after[0:1],
        jnp.where(t_row == tokens - 1, after[1:2], pltpu.roll(d_conv, tokens - 2, 0)),
    )
    d_v = tap[2] * d_conv + tap[1] * one_on + tap[0] * two_on
    grad_c[...] = (d_v * x_in[...].astype(F32)).astype(BF)
    grad_x[...] = (d_v * c_gate[...].astype(F32)).astype(BF)
    wait_bytes(outs_in.at[pl.ds(0, PLANE - 1)], o_in)

    def sum_plane(p, c):
        acc = outs[cell, p].astype(F32)
        for j in range(1, PLANE):
            acc += outs_in[(cell + j) % PLANE, p].astype(F32)
        plane_sum[p] = acc.astype(BF)
        return c

    lax.fori_loop(0, PLANES, sum_plane, 0)

    def send_sum(i, c):
        to = (z + i) % PLANES
        pltpu.make_async_remote_copy(
            plane_sum.at[to], plane_in.at[z], q_out, q_in, device_id=device(to * PLANE + cell, y)
        ).start()
        return c

    lax.fori_loop(1, PLANES, send_sum, 0)
    lax.fori_loop(3, 4, weight_grads, 0)
    wait_bytes(plane_in.at[pl.ds(0, PLANES - 1)], q_in)
    acc = plane_sum[z].astype(F32)
    for i in range(1, PLANES):
        acc += plane_in[(z + i) % PLANES].astype(F32)
    grad_out[...] = acc

    wait_bytes(got.at[0, pl.ds(0, len(FAR) * PLANE)], z_out)
    for n in range(len(NEAR)):
        wait_bytes(full_blocks(n), f_out.at[n])
    for k in range(4):
        wait_bytes(got.at[0, pl.ds(0, (PLANE if k < 2 else mid) * len(FAR))], y_out.at[k])
    for k in range(2):
        wait_bytes(part.at[0, pl.ds(0, SP // 2)], a_out.at[k])
        wait_bytes(part.at[0], b_out.at[k])
        edge_copy(k, 1).wait_send()
    wait_bytes(part.at[0, pl.ds(0, SP - 1)], r_out)
    for copy in sends:
        copy.wait_send()
    wait_bytes(outs_in.at[pl.ds(0, PLANE - 1)], o_out)
    wait_bytes(plane_in.at[pl.ds(0, PLANES - 1)], q_out)


def per_device(
    hidden_in, cotangent, routes, routing_weights, w_gate, w_up, w_down, b_gate, c_gate, x_in, taps, w_out
):
    tokens, width = hidden_in.shape
    share, ff, short = width // TP, w_gate.shape[2], x_in.shape[1]
    half = share // 2
    slots, out_rows = SP * ROWS, width // SP
    like, dma = jax.ShapeDtypeStruct, pltpu.SemaphoreType.DMA
    hbm = pl.BlockSpec(memory_space=pl.ANY)
    outs = pl.pallas_call(
        kernel,
        out_shape=(
            like((width, ff), BF),
            like((width, ff), BF),
            like((ff, width), BF),
            like((out_rows, short), F32),
            like((tokens, share), BF),
            like((tokens, short), BF),
            like((tokens, short), BF),
            like((tokens, short), BF),
        ),
        in_specs=[VMEM] * 3 + [hbm] * 9,
        out_specs=(VMEM,) * 8,
        scratch_shapes=[
            pltpu.VMEM((tokens, width), BF),
            pltpu.VMEM((tokens, width), BF),
            pltpu.VMEM((width, ff), BF),
            pltpu.VMEM((width, ff), BF),
            pltpu.VMEM((ff, width), BF),
            pltpu.VMEM((width, short), BF),
            pltpu.VMEM((tokens, short), BF),
            pltpu.VMEM((tokens, short), BF),
            pltpu.VMEM((tokens, short), BF),
            pltpu.VMEM((SP, ROWS, share), BF),
            pltpu.VMEM((len(NEAR), TP, PLANE, ROWS, share), BF),
            pltpu.VMEM((slots, tokens), BF),
            pltpu.VMEM((TP, SP, ROWS, share), BF),
            pltpu.VMEM((TP, SP, ROWS, half), BF),
            pltpu.VMEM((2, PLANES, PLANE // 2, ROWS, half), BF),
            pltpu.VMEM((2, PLANES, PLANE, ROWS, half), BF),
            pltpu.VMEM((SP, ROWS, half), BF),
            pltpu.VMEM((SP, ROWS, half), BF),
            pltpu.VMEM((slots, 2 * ff), BF),
            pltpu.VMEM((slots, ff), BF),
            pltpu.VMEM((TP, tokens, share), BF),
            pltpu.VMEM((tokens, short), BF),
            pltpu.VMEM((2, 8, short), F32),
            pltpu.VMEM((2, 8, short), F32),
            pltpu.VMEM((PLANE, PLANES, out_rows, short), BF),
            pltpu.VMEM((PLANE, PLANES, out_rows, short), BF),
            pltpu.VMEM((PLANES, out_rows, short), BF),
            pltpu.VMEM((PLANES, out_rows, short), BF),
            dma((9,)),
            dma((PLANES,)),
            dma(()),
            dma((len(NEAR),)),
            dma((len(NEAR),)),
            dma((4, PLANES)),
            dma((4,)),
            dma((2, PLANES)),
            dma((2,)),
            dma((2, PLANES)),
            dma((2,)),
            dma(()),
            dma(()),
            dma((2,)),
            dma((2,)),
            dma((6,)),
            dma((6,)),
            dma(()),
            dma(()),
            dma(()),
            dma(()),
        ],
        compiler_params=pltpu.CompilerParams(
            collective_id=0, has_side_effects=True, vmem_limit_bytes=44 * 2**20
        ),
        name="layer",
    )(
        routes.T, routing_weights.T, taps,
        *[
            pltpu.with_memory_space_constraint(v, pltpu.HBM)
            for v in (hidden_in, cotangent, w_gate[0], w_up[0], w_down[0], w_out, b_gate, c_gate, x_in)
        ],
    )
    grad_gate, grad_up, grad_down, grad_out, residual, grad_b, grad_c, grad_x = outs
    return grad_gate[None], grad_up[None], grad_down[None], grad_out, residual, grad_b, grad_c, grad_x


def solution(mesh):
    seq, both = P("sp", None), P("sp", "tp")
    return jax.shard_map(
        per_device,
        mesh=mesh,
        in_specs=(
            seq,
            seq,
            seq,
            seq,
            P("sp", None, "tp"),
            P("sp", None, "tp"),
            P("sp", "tp", None),
            both,
            both,
            both,
            P(None, "tp"),
            P(None, "tp"),
        ),
        out_specs=(
            P("sp", None, "tp"),
            P("sp", None, "tp"),
            P("sp", "tp", None),
            both,
            both,
            both,
            both,
            both,
        ),
        check_vma=False,
    )
```

```python
import functools

import jax
import jax.numpy as jnp
from jax import lax
from jax.experimental import pallas as pl
from jax.experimental.pallas import tpu as pltpu
from jax.sharding import PartitionSpec as P

PLANES, PLANE, TP, CAP = 8, 8, 4, 12
SP = PLANES * PLANE
ROWS = 2 * CAP
VMEM = pl.BlockSpec(memory_space=pltpu.VMEM)
BF, F32 = jnp.bfloat16, jnp.float32


def dot(a, b, dims=((1,), (0,))):
    return lax.dot_general(a, b, (dims, ((), ())), preferred_element_type=F32)


def device(sp, tp):
    return {"sp": sp, "tp": tp}


STEPS = (0, 2, 6, 3, 5, 4, 1, 7)
NEAR = (0, 6, 7)
FAR = range(1, 6)
NEAR_AT = 3


def plane_step(g):
    if isinstance(g, int):
        return STEPS[g]
    return sum(jnp.where(g == i, step, 0) for i, step in enumerate(STEPS))


def greet_all(me, y, right, left):
    barrier = pltpu.get_barrier_semaphore()

    def signal(i, c):
        pl.semaphore_signal(barrier, inc=1, device_id=device((me + i) % SP, y))
        return c

    lax.fori_loop(1, SP, signal, 0)
    pl.semaphore_signal(barrier, inc=1, device_id=device(me, right))
    pl.semaphore_signal(barrier, inc=1, device_id=device(me, left))
    return barrier


def wait_bytes(ref, sem):
    pltpu.make_async_copy(ref, ref, sem).wait()


def kernel(
    routes, weights, taps, hidden_hbm, cot_hbm, w_gate_hbm, w_up_hbm, w_down_hbm, w_out_hbm, b_hbm, c_hbm, x_hbm,
    grad_gate, grad_up, grad_down, grad_out, residual, small,
    hidden, cot, w_gate, w_up, w_down, w_out, b_gate, c_gate, x_in,
    send, own, select, got, part, near_in, total_in, sums, back, d_both, hid_rows, full, y_short,
    edge, edge_in, outs, pair_in, pair_sum, outs_in, plane_sum, plane_in,
    ld, z_in, z_out, f_in, f_out, y_in, y_out, a_in, a_out, b_in, b_out, r_in, r_out,
    h_in, h_out, e_in, e_out, p_in, p_out, o_in, o_out, q_in, q_out,
):
    me, y = lax.axis_index("sp"), lax.axis_index("tp")
    z, cell = me // PLANE, me % PLANE
    right, left, far = (y + 1) % TP, (y + 3) % TP, (y + 2) % TP
    tokens, width = hidden.shape
    share = width // TP
    half_share = share // 2
    part_rows = PLANE * ROWS
    slots = SP * ROWS
    mid = PLANE // 2
    ff = w_gate.shape[1]
    out_rows = grad_out.shape[0]

    barrier = greet_all(me, y, right, left)
    loads = [
        pltpu.make_async_copy(a, b, ld.at[i])
        for i, (a, b) in enumerate(
            (
                (hidden_hbm, hidden),
                (cot_hbm, cot),
                (c_hbm, c_gate),
                (x_hbm, x_in),
                (w_gate_hbm, w_gate),
                (w_up_hbm, w_up),
                (w_down_hbm, w_down),
                (b_hbm, b_gate),
                (w_out_hbm, w_out),
            )
        )
    ]
    for load in loads:
        load.start()

    down = lax.broadcasted_iota(jnp.int32, (tokens, tokens), 0)
    across = lax.broadcasted_iota(jnp.int32, (tokens, tokens), 1)

    def count(match):
        return jnp.sum(jnp.where(match, 1.0, 0.0), axis=0, keepdims=True).astype(jnp.int32)

    r0, r1 = routes[0:1, :], routes[1:2, :]
    w0, w1 = weights[0:1, :], weights[1:2, :]
    c0 = jnp.sum(jnp.where(down == across, r0, 0), axis=1, keepdims=True)
    c1 = jnp.sum(jnp.where(down == across, r1, 0), axis=1, keepdims=True)
    earlier = down < across
    t0 = r0 * ROWS + count(earlier & (c0 == r0))
    t1 = r1 * ROWS + count(c0 == r1) + count(earlier & (c1 == r1))
    row = lax.broadcasted_iota(jnp.int32, (part_rows, tokens), 0)
    is_token = lax.broadcasted_iota(jnp.int32, (part_rows, 1), 0) % ROWS < CAP

    def picks(plane):
        slot = row + plane * part_rows
        h = jnp.where((t0 == slot) | (t1 == slot), 1.0, 0.0)
        s0, s1 = t0 + CAP == slot, t1 + CAP == slot
        s = jnp.where(s0 | s1, 1.0, 0.0)
        scale = jnp.sum(jnp.where(s0, w0, 0.0) + jnp.where(s1, w1, 0.0), axis=1, keepdims=True)
        select[pl.ds(pl.multiple_of(plane * part_rows, part_rows), part_rows), :] = (h + s).astype(BF)
        return h.astype(BF), s.astype(BF), jnp.where(is_token, 1.0, scale)

    def plane_of(g, sign):
        return (z + sign * plane_step(g) + PLANES) % PLANES

    mine = pl.ds(pl.multiple_of(y * share, share), share)

    def pack(g):
        plane = plane_of(g, 1)
        h, s, scale = picks(plane)
        rows = (dot(h, hidden[:, mine]) + dot(s, cot[:, mine])) * scale
        send[pl.ds(plane * PLANE, PLANE)] = rows.astype(BF).reshape(PLANE, ROWS, share)

    def send_group(g):
        def one(j, c):
            to = plane_of(g, 1) * PLANE + (cell + j) % PLANE
            pltpu.make_async_remote_copy(
                send.at[to], got.at[y, me], z_out, z_in.at[g], device_id=device(to, y)
            ).start()
            return c

        lax.fori_loop(0, PLANE, one, 0)

    loads[0].wait()
    loads[1].wait()
    def pack_full(n):
        plane = plane_of(NEAR[n], 1)
        h, s, scale = picks(plane)
        for k in range(TP):
            cols = pl.ds(k * share, share)
            rows = (dot(h, hidden[:, cols]) + dot(s, cot[:, cols])) * scale
            own[n, k] = rows.astype(BF).reshape(PLANE, ROWS, share)

    def send_full(n, first):
        count = PLANE - first

        def one(i, c):
            j, k = (cell + first + i % count) % PLANE, i // count
            to = plane_of(NEAR[n], 1) * PLANE + j
            pltpu.make_async_remote_copy(
                own.at[n, k, j], got.at[k, me], f_out.at[n], f_in.at[n], device_id=device(to, y)
            ).start()
            return c

        lax.fori_loop(0, TP * count, one, 0)

    lax.fori_loop(1, 3, lambda g, c: (pack(g), c)[1], 0)
    pl.semaphore_wait(barrier, SP + 1)
    lax.fori_loop(1, 3, lambda g, c: (send_group(g), c)[1], 0)
    lax.fori_loop(3, FAR[-1] + 1, lambda g, c: (pack(g), c)[1], 0)
    pack_full(0)
    for k in range(TP):
        got[k, me] = own[0, k, cell]
    lax.fori_loop(3, FAR[-1] + 1, lambda g, c: (send_group(g), c)[1], 0)
    send_full(0, 1)
    pack_full(1)
    pack_full(2)

    loads[2].wait()
    loads[3].wait()
    edge[0] = c_gate[tokens - 8 :, :].astype(F32) * x_in[tokens - 8 :, :].astype(F32)

    def edge_copy(k, by):
        return pltpu.make_async_remote_copy(
            edge.at[k], edge_in.at[k], h_out.at[k], h_in.at[k], device_id=device((me + by + SP) % SP, y)
        )

    edge_copy(0, 1).start()
    for load in loads[4:7]:
        load.wait()

    def block(k, g, at=0, size=PLANE):
        return got.at[k, pl.ds(plane_of(g, -1) * PLANE + at, size)]

    def pass_on(s, g, k, to):
        ref = block(s, g) if k < 2 else block(s, g, (k - 2) * mid, mid)
        return pltpu.make_async_remote_copy(
            ref, ref, y_out.at[k], y_in.at[k, g], device_id=device(me, to)
        )

    def expert_rows(g):
        plane = plane_of(g, -1)
        blocks = pl.ds(plane * PLANE, PLANE)
        pre_gate = pre_up = d_hid = jnp.zeros((part_rows, ff), F32)
        for k in range(TP):
            x = got[k, blocks].reshape(part_rows, share)
            cols = pl.ds(k * share, share)
            pre_gate += dot(x, w_gate[cols, :])
            pre_up += dot(x, w_up[cols, :])
            d_hid += dot(x, w_down[:, cols], ((1,), (1,)))
        d_hid = pltpu.roll(d_hid, part_rows - CAP, 0)
        sigma = 1.0 / (1.0 + jnp.exp(-pre_gate))
        silu = pre_gate * sigma
        d_up = d_hid * silu
        d_pre = d_hid * pre_up * sigma * (1.0 + pre_gate * (1.0 - sigma))
        twice_pre = jnp.where(is_token, d_pre, pltpu.roll(d_pre, CAP, 0)).astype(BF)
        twice_up = jnp.where(is_token, d_up, pltpu.roll(d_up, CAP, 0)).astype(BF)
        for k in range(TP):
            cols = pl.ds(k * share, share)
            grad = dot(twice_pre, w_gate[cols, :], ((1,), (1,)))
            grad += dot(twice_up, w_up[cols, :], ((1,), (1,)))
            folded = jnp.where(is_token, grad[:, :half_share], grad[:, half_share:])
            part[k, blocks] = folded.astype(BF).reshape(PLANE, ROWS, half_share)
        at = pl.ds(pl.multiple_of(plane * part_rows, part_rows), part_rows)
        d_both[at, 0:ff] = jnp.where(is_token, d_pre, 0.0).astype(BF)
        d_both[at, ff:] = jnp.where(is_token, d_up, 0.0).astype(BF)
        hid_rows[at, :] = jnp.where(is_token, 0.0, pltpu.roll(silu * pre_up, CAP, 0)).astype(BF)

    def far_half(g, k, to):
        at = plane_of(g, -1) * PLANE + k * mid
        return pltpu.make_async_remote_copy(
            part.at[far, pl.ds(at, mid)], near_in.at[k, g], a_out.at[k], a_in.at[k, g],
            device_id=device(me, to),
        )

    def near_sum(g, k, to):
        return pltpu.make_async_remote_copy(
            part.at[to, pl.ds(plane_of(g, -1) * PLANE, PLANE)], total_in.at[k, g], b_out.at[k],
            b_in.at[k, g], device_id=device(me, to),
        )

    def add(g, k, to):
        at = pl.ds(plane_of(g, -1) * PLANE + k * mid, mid)
        part[to, at] = (part[to, at].astype(F32) + near_in[k, g].astype(F32)).astype(BF)

    def send_back(g, j):
        to = plane_of(g, -1) * PLANE + (cell + j) % PLANE
        pltpu.make_async_remote_copy(
            sums.at[to], back.at[me], r_out, r_in, device_id=device(to, y)
        ).start()

    def full_blocks(n):
        return got.at[0, pl.ds(0, TP * (PLANE - 1 if n == 0 else PLANE))]

    def step(t, c):
        @pl.when(t == NEAR_AT)
        def _():
            send_full(1, 0)
            send_full(2, 0)

        @pl.when(t <= FAR[-1])
        def _():
            wait_bytes(block(y, t), z_in.at[t])
            pass_on(y, t, 0, right).start()
            pass_on(y, t, 1, left).start()

        @pl.when((t > 1) & (t <= FAR[-1] + 1))
        def _():
            g = t - 1
            pass_on(left, g, 0, left).wait_recv()
            pass_on(left, g, 2, right).start()
            pass_on(right, g, 1, right).wait_recv()
            pass_on(right, g, 3, left).start()

        @pl.when((t >= 4) & (t < PLANES + 4))
        def _():
            g = t - 4
            far_half(g, 0, right).wait_recv()
            add(g, 0, right)
            far_half(g, 1, left).wait_recv()
            add(g, 1, left)

        @pl.when(t >= 6)
        def _():
            g = t - 6

            @pl.when(g > 0)
            def _():
                send_back(g, 0)

            lax.fori_loop(1, PLANE, lambda j, d: (send_back(g, j), d)[1], 0)

        @pl.when((t >= 4) & (t < PLANES + 4))
        def _():
            near_sum(t - 4, 0, right).start()
            near_sum(t - 4, 1, left).start()

        @pl.when((t >= 5) & (t < PLANES + 5))
        def _():
            g = t - 5
            near_sum(g, 0, right).wait_recv()
            near_sum(g, 1, left).wait_recv()
            at = pl.ds(plane_of(g, -1) * PLANE, PLANE)
            sums[at] = (
                part[y, at].astype(F32) + total_in[0, g].astype(F32) + total_in[1, g].astype(F32)
            ).astype(BF)

        for n, g in enumerate(NEAR):

            @pl.when(t == g + 2)
            def _():
                wait_bytes(full_blocks(n), f_in.at[n])

        @pl.when((t > 2) & (t <= FAR[-1] + 2))
        def _():
            pass_on(far, t - 2, 2, right).wait_recv()
            pass_on(far, t - 2, 3, left).wait_recv()

        @pl.when((t >= 2) & (t < PLANES + 2))
        def _():
            expert_rows(t - 2)
            far_half(t - 2, 0, right).start()
            far_half(t - 2, 1, left).start()

        return c

    lax.fori_loop(1, PLANES + 6, step, 0)
    back[me] = sums[me]

    wait_bytes(part.at[0, pl.ds(0, SP - 1)], r_in)
    token_slot = lax.broadcasted_iota(jnp.int32, (slots, 1), 0) % ROWS < CAP
    rows = back[...].reshape(slots, half_share)
    zero = jnp.zeros_like(rows)
    kept = jnp.concatenate(
        [jnp.where(token_slot, rows, zero), jnp.where(token_slot, zero, rows)], axis=1
    )
    total = (cot[:, mine].astype(F32) + dot(select[...], kept, ((0,), (0,)))).astype(BF)
    full[y] = total
    residual[...] = total

    rows_half = tokens // 2

    def spread(s, at, k, to):
        ref = full.at[s, pl.ds(at * rows_half, rows_half)]
        return pltpu.make_async_remote_copy(
            ref, ref, e_out.at[k], e_in.at[k], device_id=device(me, to)
        )

    def weight_grads(k, c):
        rows = got[k].reshape(slots, share)
        at = pl.ds(pl.multiple_of(k * share, share), share)
        both = dot(rows, d_both[...], ((0,), (0,)))
        grad_gate[at, :] = both[:, :ff].astype(BF)
        grad_up[at, :] = both[:, ff:].astype(BF)
        grad_down[:, at] = dot(hid_rows[...], rows, ((0,), (0,))).astype(BF)
        return c

    sends = [spread(y, 0, 0, right), spread(y, 1, 1, left), spread(y, 1, 2, right), spread(y, 0, 3, left)]
    for copy in sends:
        copy.start()
    t_row = lax.broadcasted_iota(jnp.int32, (tokens, 1), 0)
    tap = [taps[i : i + 1, :].astype(F32) for i in range(3)]
    gated = c_gate[...].astype(F32) * x_in[...].astype(F32)
    edge_copy(0, 1).wait_recv()
    before = jnp.where(me == 0, 0.0, edge_in[0])
    one_back = jnp.where(t_row == 0, before[7:8], pltpu.roll(gated, 1, 0))
    two_back = jnp.where(
        t_row == 0, before[6:7], jnp.where(t_row == 1, before[7:8], pltpu.roll(gated, 2, 0))
    )
    conv = tap[0] * two_back + tap[1] * one_back + tap[2] * gated
    loads[7].wait()
    b_f = b_gate[...].astype(F32)
    y_short[...] = (b_f * conv).astype(BF)
    loads[8].wait()

    def project(k):
        grad = dot(full[k], y_short[...], ((0,), (0,))).astype(BF)
        for zz in range(2):
            for j in range(PLANE):
                at = (zz * PLANE + j) * out_rows
                outs[j % 2, j // 2, 2 * k + zz] = grad[at : at + out_rows]
        return dot(full[k], w_out[pl.ds(pl.multiple_of(k * share, share), share), :])

    core, x_at = cell % 2, cell // 2
    chips = PLANE // 2

    def to_partner(k):
        return pltpu.make_async_remote_copy(
            outs.at[1 - core, :, pl.ds(2 * k, 2)], pair_in.at[:, pl.ds(2 * k, 2)], p_out.at[k], p_in.at[k],
            device_id=device(z * PLANE + x_at * 2 + 1 - core, y),
        )

    def send_out(k):
        to_partner(k).wait_recv()
        at = pl.ds(2 * k, 2)
        pair_sum[:, at] = (outs[core, :, at].astype(F32) + pair_in[:, at].astype(F32)).astype(BF)
        for j in range(1, chips):
            to = (x_at + j) % chips
            pltpu.make_async_remote_copy(
                pair_sum.at[to, at], outs_in.at[x_at, at], o_out, o_in,
                device_id=device(z * PLANE + to * 2 + core, y),
            ).start()

    d_y = project(y)
    to_partner(y).start()
    lax.fori_loop(0, 1, weight_grads, 0)
    send_out(y)
    spread(left, 0, 0, left).wait_recv()
    sends.append(spread(left, 0, 4, right))
    sends[-1].start()
    spread(right, 1, 1, right).wait_recv()
    sends.append(spread(right, 1, 5, left))
    sends[-1].start()
    spread(left, 1, 2, left).wait_recv()
    d_y += project(left)
    to_partner(left).start()
    spread(right, 0, 3, right).wait_recv()
    d_y += project(right)
    to_partner(right).start()
    send_out(left)
    send_out(right)
    lax.fori_loop(1, 2, weight_grads, 0)
    spread(far, 0, 4, right).wait_recv()
    spread(far, 1, 5, left).wait_recv()
    d_y += project(far)
    to_partner(far).start()
    d_conv = b_f * d_y
    edge[1] = d_conv[0:8]
    small[0] = (d_y * conv).astype(BF)
    edge_copy(1, -1).start()
    send_out(far)
    lax.fori_loop(2, 3, weight_grads, 0)
    edge_copy(1, -1).wait_recv()
    after = jnp.where(me == SP - 1, 0.0, edge_in[1])
    one_on = jnp.where(t_row == tokens - 1, after[0:1], pltpu.roll(d_conv, tokens - 1, 0))
    two_on = jnp.where(
        t_row == tokens - 2,
        after[0:1],
        jnp.where(t_row == tokens - 1, after[1:2], pltpu.roll(d_conv, tokens - 2, 0)),
    )
    d_v = tap[2] * d_conv + tap[1] * one_on + tap[0] * two_on
    small[1] = (d_v * x_in[...].astype(F32)).astype(BF)
    small[2] = (d_v * c_gate[...].astype(F32)).astype(BF)
    wait_bytes(outs_in.at[pl.ds(0, chips - 1)], o_in)

    def sum_plane(p, c):
        acc = pair_sum[x_at, p].astype(F32)
        for j in range(1, chips):
            acc += outs_in[(x_at + j) % chips, p].astype(F32)
        plane_sum[p] = acc.astype(BF)
        return c

    lax.fori_loop(0, PLANES, sum_plane, 0)

    def send_sum(i, c):
        to = (z + i) % PLANES
        pltpu.make_async_remote_copy(
            plane_sum.at[to], plane_in.at[z], q_out, q_in, device_id=device(to * PLANE + cell, y)
        ).start()
        return c

    lax.fori_loop(1, PLANES, send_sum, 0)
    lax.fori_loop(3, 4, weight_grads, 0)
    wait_bytes(plane_in.at[pl.ds(0, PLANES - 1)], q_in)
    acc = plane_sum[z].astype(F32)
    for i in range(1, PLANES):
        acc += plane_in[(z + i) % PLANES].astype(F32)
    grad_out[...] = acc

    wait_bytes(got.at[0, pl.ds(0, len(FAR) * PLANE)], z_out)
    for n in range(len(NEAR)):
        wait_bytes(full_blocks(n), f_out.at[n])
    for k in range(4):
        wait_bytes(got.at[0, pl.ds(0, (PLANE if k < 2 else mid) * len(FAR))], y_out.at[k])
    for k in range(2):
        wait_bytes(part.at[0, pl.ds(0, SP // 2)], a_out.at[k])
        wait_bytes(part.at[0], b_out.at[k])
        edge_copy(k, 1).wait_send()
    wait_bytes(part.at[0, pl.ds(0, SP - 1)], r_out)
    for copy in sends:
        copy.wait_send()
    wait_bytes(outs_in.at[pl.ds(0, chips - 1)], o_out)
    for k in range(TP):
        to_partner(k).wait_send()
    wait_bytes(plane_in.at[pl.ds(0, PLANES - 1)], q_out)


def per_device(
    hidden_in, cotangent, routes, routing_weights, w_gate, w_up, w_down, b_gate, c_gate, x_in, taps, w_out
):
    tokens, width = hidden_in.shape
    share, ff, short = width // TP, w_gate.shape[2], x_in.shape[1]
    half = share // 2
    slots, out_rows = SP * ROWS, width // SP
    like, dma = jax.ShapeDtypeStruct, pltpu.SemaphoreType.DMA
    hbm = pl.BlockSpec(memory_space=pl.ANY)
    outs = pl.pallas_call(
        kernel,
        out_shape=(
            like((width, ff), BF),
            like((width, ff), BF),
            like((ff, width), BF),
            like((out_rows, short), F32),
            like((tokens, share), BF),
            like((3, tokens, short), BF),
        ),
        in_specs=[VMEM] * 3 + [hbm] * 9,
        out_specs=(VMEM,) * 6,
        scratch_shapes=[
            pltpu.VMEM((tokens, width), BF),
            pltpu.VMEM((tokens, width), BF),
            pltpu.VMEM((width, ff), BF),
            pltpu.VMEM((width, ff), BF),
            pltpu.VMEM((ff, width), BF),
            pltpu.VMEM((width, short), BF),
            pltpu.VMEM((tokens, short), BF),
            pltpu.VMEM((tokens, short), BF),
            pltpu.VMEM((tokens, short), BF),
            pltpu.VMEM((SP, ROWS, share), BF),
            pltpu.VMEM((len(NEAR), TP, PLANE, ROWS, share), BF),
            pltpu.VMEM((slots, tokens), BF),
            pltpu.VMEM((TP, SP, ROWS, share), BF),
            pltpu.VMEM((TP, SP, ROWS, half), BF),
            pltpu.VMEM((2, PLANES, PLANE // 2, ROWS, half), BF),
            pltpu.VMEM((2, PLANES, PLANE, ROWS, half), BF),
            pltpu.VMEM((SP, ROWS, half), BF),
            pltpu.VMEM((SP, ROWS, half), BF),
            pltpu.VMEM((slots, 2 * ff), BF),
            pltpu.VMEM((slots, ff), BF),
            pltpu.VMEM((TP, tokens, share), BF),
            pltpu.VMEM((tokens, short), BF),
            pltpu.VMEM((2, 8, short), F32),
            pltpu.VMEM((2, 8, short), F32),
            pltpu.VMEM((2, PLANE // 2, PLANES, out_rows, short), BF),
            pltpu.VMEM((PLANE // 2, PLANES, out_rows, short), BF),
            pltpu.VMEM((PLANE // 2, PLANES, out_rows, short), BF),
            pltpu.VMEM((PLANE // 2, PLANES, out_rows, short), BF),
            pltpu.VMEM((PLANES, out_rows, short), BF),
            pltpu.VMEM((PLANES, out_rows, short), BF),
            dma((9,)),
            dma((PLANES,)),
            dma(()),
            dma((len(NEAR),)),
            dma((len(NEAR),)),
            dma((4, PLANES)),
            dma((4,)),
            dma((2, PLANES)),
            dma((2,)),
            dma((2, PLANES)),
            dma((2,)),
            dma(()),
            dma(()),
            dma((2,)),
            dma((2,)),
            dma((6,)),
            dma((6,)),
            dma((TP,)),
            dma((TP,)),
            dma(()),
            dma(()),
            dma(()),
            dma(()),
        ],
        compiler_params=pltpu.CompilerParams(
            collective_id=0, has_side_effects=True, vmem_limit_bytes=44 * 2**20
        ),
        name="layer",
    )(
        routes.T, routing_weights.T, taps,
        *[
            pltpu.with_memory_space_constraint(v, pltpu.HBM)
            for v in (hidden_in, cotangent, w_gate[0], w_up[0], w_down[0], w_out, b_gate, c_gate, x_in)
        ],
    )
    grad_gate, grad_up, grad_down, grad_out, residual, small = outs
    grad_b, grad_c, grad_x = small[0], small[1], small[2]
    return grad_gate[None], grad_up[None], grad_down[None], grad_out, residual, grad_b, grad_c, grad_x


def solution(mesh):
    seq, both = P("sp", None), P("sp", "tp")
    return jax.shard_map(
        per_device,
        mesh=mesh,
        in_specs=(
            seq,
            seq,
            seq,
            seq,
            P("sp", None, "tp"),
            P("sp", None, "tp"),
            P("sp", "tp", None),
            both,
            both,
            both,
            P(None, "tp"),
            P(None, "tp"),
        ),
        out_specs=(
            P("sp", None, "tp"),
            P("sp", None, "tp"),
            P("sp", "tp", None),
            both,
            both,
            both,
            both,
            both,
        ),
        check_vma=False,
    )
```

```python
import functools

import jax
import jax.numpy as jnp
from jax import lax
from jax.experimental import pallas as pl
from jax.experimental.pallas import tpu as pltpu
from jax.sharding import PartitionSpec as P

PLANES, PLANE, TP, CAP = 8, 8, 4, 12
SP = PLANES * PLANE
ROWS = 2 * CAP
VMEM = pl.BlockSpec(memory_space=pltpu.VMEM)
BF, F32 = jnp.bfloat16, jnp.float32


def dot(a, b, dims=((1,), (0,))):
    return lax.dot_general(a, b, (dims, ((), ())), preferred_element_type=F32)


def device(sp, tp):
    return {"sp": sp, "tp": tp}


STEPS = (0, 2, 6, 3, 5, 4, 1, 7)
NEAR = (0, 6, 7)
FAR = range(1, 6)
NEAR_AT = 3


def plane_step(g):
    if isinstance(g, int):
        return STEPS[g]
    return sum(jnp.where(g == i, step, 0) for i, step in enumerate(STEPS))


def greet_all(me, y, right, left):
    barrier = pltpu.get_barrier_semaphore()

    def signal(i, c):
        pl.semaphore_signal(barrier, inc=1, device_id=device((me + i) % SP, y))
        return c

    lax.fori_loop(1, SP, signal, 0)
    pl.semaphore_signal(barrier, inc=1, device_id=device(me, right))
    pl.semaphore_signal(barrier, inc=1, device_id=device(me, left))
    return barrier


def wait_bytes(ref, sem):
    pltpu.make_async_copy(ref, ref, sem).wait()


def kernel(
    routes, weights, taps, hidden_hbm, cot_hbm, w_gate_hbm, w_up_hbm, w_down_hbm, w_out_hbm, b_hbm, c_hbm, x_hbm,
    grad_gate, grad_up, grad_down, grad_out, residual, small,
    hidden, cot, w_gate, w_up, w_down, w_out, b_gate, c_gate, x_in,
    send, own, select, got, part, near_in, total_in, sums, back, d_both, hid_rows, full, y_short,
    edge, edge_in, outs, pair_in, pair_sum, outs_in, plane_sum, plane_in,
    ld, z_in, z_out, f_in, f_out, y_in, y_out, a_in, a_out, b_in, b_out, r_in, r_out,
    h_in, h_out, e_in, e_out, p_in, p_out, o_in, o_out, q_in, q_out,
):
    me, y = lax.axis_index("sp"), lax.axis_index("tp")
    z, cell = me // PLANE, me % PLANE
    right, left, far = (y + 1) % TP, (y + 3) % TP, (y + 2) % TP
    tokens, width = hidden.shape
    share = width // TP
    half_share = share // 2
    part_rows = PLANE * ROWS
    slots = SP * ROWS
    mid = PLANE // 2
    ff = w_gate.shape[1]
    out_rows = grad_out.shape[0]

    barrier = greet_all(me, y, right, left)
    loads = [
        pltpu.make_async_copy(a, b, ld.at[i])
        for i, (a, b) in enumerate(
            (
                (hidden_hbm, hidden),
                (cot_hbm, cot),
                (c_hbm, c_gate),
                (x_hbm, x_in),
                (w_gate_hbm, w_gate),
                (w_up_hbm, w_up),
                (w_down_hbm, w_down),
                (b_hbm, b_gate),
                (w_out_hbm, w_out),
            )
        )
    ]
    for load in loads:
        load.start()

    down = lax.broadcasted_iota(jnp.int32, (tokens, tokens), 0)
    across = lax.broadcasted_iota(jnp.int32, (tokens, tokens), 1)

    def count(match):
        return jnp.sum(jnp.where(match, 1.0, 0.0), axis=0, keepdims=True).astype(jnp.int32)

    r0, r1 = routes[0:1, :], routes[1:2, :]
    w0, w1 = weights[0:1, :], weights[1:2, :]
    c0 = jnp.sum(jnp.where(down == across, r0, 0), axis=1, keepdims=True)
    c1 = jnp.sum(jnp.where(down == across, r1, 0), axis=1, keepdims=True)
    earlier = down < across
    t0 = r0 * ROWS + count(earlier & (c0 == r0))
    t1 = r1 * ROWS + count(c0 == r1) + count(earlier & (c1 == r1))
    row = lax.broadcasted_iota(jnp.int32, (part_rows, tokens), 0)
    is_token = lax.broadcasted_iota(jnp.int32, (part_rows, 1), 0) % ROWS < CAP

    def picks(plane):
        slot = row + plane * part_rows
        h = jnp.where((t0 == slot) | (t1 == slot), 1.0, 0.0)
        s0, s1 = t0 + CAP == slot, t1 + CAP == slot
        s = jnp.where(s0 | s1, 1.0, 0.0)
        scale = jnp.sum(jnp.where(s0, w0, 0.0) + jnp.where(s1, w1, 0.0), axis=1, keepdims=True)
        select[pl.ds(pl.multiple_of(plane * part_rows, part_rows), part_rows), :] = (h + s).astype(BF)
        return h.astype(BF), s.astype(BF), jnp.where(is_token, 1.0, scale)

    def plane_of(g, sign):
        return (z + sign * plane_step(g) + PLANES) % PLANES

    mine = pl.ds(pl.multiple_of(y * share, share), share)

    def pack(g):
        plane = plane_of(g, 1)
        h, s, scale = picks(plane)
        rows = (dot(h, hidden[:, mine]) + dot(s, cot[:, mine])) * scale
        send[pl.ds(plane * PLANE, PLANE)] = rows.astype(BF).reshape(PLANE, ROWS, share)

    def send_group(g):
        def one(j, c):
            to = plane_of(g, 1) * PLANE + (cell + j) % PLANE
            pltpu.make_async_remote_copy(
                send.at[to], got.at[y, me], z_out, z_in.at[g], device_id=device(to, y)
            ).start()
            return c

        lax.fori_loop(0, PLANE, one, 0)

    loads[0].wait()
    loads[1].wait()
    def pack_full(n):
        plane = plane_of(NEAR[n], 1)
        h, s, scale = picks(plane)
        for k in range(TP):
            cols = pl.ds(k * share, share)
            rows = (dot(h, hidden[:, cols]) + dot(s, cot[:, cols])) * scale
            own[n, k] = rows.astype(BF).reshape(PLANE, ROWS, share)

    def send_full(n, first):
        count = PLANE - first

        def one(i, c):
            j, k = (cell + first + i % count) % PLANE, i // count
            to = plane_of(NEAR[n], 1) * PLANE + j
            pltpu.make_async_remote_copy(
                own.at[n, k, j], got.at[k, me], f_out.at[n], f_in.at[n], device_id=device(to, y)
            ).start()
            return c

        lax.fori_loop(0, TP * count, one, 0)

    lax.fori_loop(1, 3, lambda g, c: (pack(g), c)[1], 0)
    pl.semaphore_wait(barrier, SP + 1)
    lax.fori_loop(1, 3, lambda g, c: (send_group(g), c)[1], 0)
    lax.fori_loop(3, FAR[-1] + 1, lambda g, c: (pack(g), c)[1], 0)
    pack_full(0)
    for k in range(TP):
        got[k, me] = own[0, k, cell]
    lax.fori_loop(3, FAR[-1] + 1, lambda g, c: (send_group(g), c)[1], 0)
    send_full(0, 1)
    pack_full(1)
    pack_full(2)

    loads[2].wait()
    loads[3].wait()
    edge[0] = c_gate[tokens - 8 :, :].astype(F32) * x_in[tokens - 8 :, :].astype(F32)

    def edge_copy(k, by):
        return pltpu.make_async_remote_copy(
            edge.at[k], edge_in.at[k], h_out.at[k], h_in.at[k], device_id=device((me + by + SP) % SP, y)
        )

    edge_copy(0, 1).start()
    for load in loads[4:7]:
        load.wait()

    def block(k, g, at=0, size=PLANE):
        return got.at[k, pl.ds(plane_of(g, -1) * PLANE + at, size)]

    def pass_on(s, g, k, to):
        ref = block(s, g) if k < 2 else block(s, g, (k - 2) * mid, mid)
        return pltpu.make_async_remote_copy(
            ref, ref, y_out.at[k], y_in.at[k, g], device_id=device(me, to)
        )

    def expert_rows(g):
        plane = plane_of(g, -1)
        blocks = pl.ds(plane * PLANE, PLANE)
        pre_gate = pre_up = d_hid = jnp.zeros((part_rows, ff), F32)
        for k in range(TP):
            x = got[k, blocks].reshape(part_rows, share)
            cols = pl.ds(k * share, share)
            pre_gate += dot(x, w_gate[cols, :])
            pre_up += dot(x, w_up[cols, :])
            d_hid += dot(x, w_down[:, cols], ((1,), (1,)))
        d_hid = pltpu.roll(d_hid, part_rows - CAP, 0)
        sigma = 1.0 / (1.0 + jnp.exp(-pre_gate))
        silu = pre_gate * sigma
        d_up = d_hid * silu
        d_pre = d_hid * pre_up * sigma * (1.0 + pre_gate * (1.0 - sigma))
        twice_pre = jnp.where(is_token, d_pre, pltpu.roll(d_pre, CAP, 0)).astype(BF)
        twice_up = jnp.where(is_token, d_up, pltpu.roll(d_up, CAP, 0)).astype(BF)
        for k in range(TP):
            cols = pl.ds(k * share, share)
            grad = dot(twice_pre, w_gate[cols, :], ((1,), (1,)))
            grad += dot(twice_up, w_up[cols, :], ((1,), (1,)))
            folded = jnp.where(is_token, grad[:, :half_share], grad[:, half_share:])
            part[k, blocks] = folded.astype(BF).reshape(PLANE, ROWS, half_share)
        at = pl.ds(pl.multiple_of(plane * part_rows, part_rows), part_rows)
        d_both[at, 0:ff] = jnp.where(is_token, d_pre, 0.0).astype(BF)
        d_both[at, ff:] = jnp.where(is_token, d_up, 0.0).astype(BF)
        hid_rows[at, :] = jnp.where(is_token, 0.0, pltpu.roll(silu * pre_up, CAP, 0)).astype(BF)

    def far_half(g, k, to):
        at = plane_of(g, -1) * PLANE + k * mid
        return pltpu.make_async_remote_copy(
            part.at[far, pl.ds(at, mid)], near_in.at[k, g], a_out.at[k], a_in.at[k, g],
            device_id=device(me, to),
        )

    def near_sum(g, k, to):
        return pltpu.make_async_remote_copy(
            part.at[to, pl.ds(plane_of(g, -1) * PLANE, PLANE)], total_in.at[k, g], b_out.at[k],
            b_in.at[k, g], device_id=device(me, to),
        )

    def add(g, k, to):
        at = pl.ds(plane_of(g, -1) * PLANE + k * mid, mid)
        part[to, at] = (part[to, at].astype(F32) + near_in[k, g].astype(F32)).astype(BF)

    def send_back(g, j):
        to = plane_of(g, -1) * PLANE + (cell + j) % PLANE
        pltpu.make_async_remote_copy(
            sums.at[to], back.at[me], r_out, r_in, device_id=device(to, y)
        ).start()

    def full_blocks(n):
        return got.at[0, pl.ds(0, TP * (PLANE - 1 if n == 0 else PLANE))]

    def step(t, c):
        @pl.when(t == NEAR_AT)
        def _():
            send_full(1, 0)
            send_full(2, 0)

        @pl.when(t <= FAR[-1])
        def _():
            wait_bytes(block(y, t), z_in.at[t])
            pass_on(y, t, 0, right).start()
            pass_on(y, t, 1, left).start()

        @pl.when((t > 1) & (t <= FAR[-1] + 1))
        def _():
            g = t - 1
            pass_on(left, g, 0, left).wait_recv()
            pass_on(left, g, 2, right).start()
            pass_on(right, g, 1, right).wait_recv()
            pass_on(right, g, 3, left).start()

        @pl.when((t >= 4) & (t < PLANES + 4))
        def _():
            g = t - 4
            far_half(g, 0, right).wait_recv()
            add(g, 0, right)
            far_half(g, 1, left).wait_recv()
            add(g, 1, left)

        @pl.when(t >= 6)
        def _():
            g = t - 6

            @pl.when(g > 0)
            def _():
                send_back(g, 0)

            lax.fori_loop(1, PLANE, lambda j, d: (send_back(g, j), d)[1], 0)

        @pl.when((t >= 4) & (t < PLANES + 4))
        def _():
            near_sum(t - 4, 0, right).start()
            near_sum(t - 4, 1, left).start()

        @pl.when((t >= 5) & (t < PLANES + 5))
        def _():
            g = t - 5
            near_sum(g, 0, right).wait_recv()
            near_sum(g, 1, left).wait_recv()
            at = pl.ds(plane_of(g, -1) * PLANE, PLANE)
            sums[at] = (
                part[y, at].astype(F32) + total_in[0, g].astype(F32) + total_in[1, g].astype(F32)
            ).astype(BF)

        for n, g in enumerate(NEAR):

            @pl.when(t == g + 2)
            def _():
                wait_bytes(full_blocks(n), f_in.at[n])

        @pl.when((t > 2) & (t <= FAR[-1] + 2))
        def _():
            pass_on(far, t - 2, 2, right).wait_recv()
            pass_on(far, t - 2, 3, left).wait_recv()

        @pl.when((t >= 2) & (t < PLANES + 2))
        def _():
            expert_rows(t - 2)
            far_half(t - 2, 0, right).start()
            far_half(t - 2, 1, left).start()

        return c

    lax.fori_loop(1, PLANES + 6, step, 0)
    back[me] = sums[me]

    wait_bytes(part.at[0, pl.ds(0, SP - 1)], r_in)
    token_slot = lax.broadcasted_iota(jnp.int32, (slots, 1), 0) % ROWS < CAP
    rows = back[...].reshape(slots, half_share)
    zero = jnp.zeros_like(rows)
    kept = jnp.concatenate(
        [jnp.where(token_slot, rows, zero), jnp.where(token_slot, zero, rows)], axis=1
    )
    total = (cot[:, mine].astype(F32) + dot(select[...], kept, ((0,), (0,)))).astype(BF)
    full[y] = total
    residual[...] = total

    rows_half = tokens // 2

    def spread(s, at, k, to):
        ref = full.at[s, pl.ds(at * rows_half, rows_half)]
        return pltpu.make_async_remote_copy(
            ref, ref, e_out.at[k], e_in.at[k], device_id=device(me, to)
        )

    def weight_grads(k, c):
        rows = got[k].reshape(slots, share)
        at = pl.ds(pl.multiple_of(k * share, share), share)
        both = dot(rows, d_both[...], ((0,), (0,)))
        grad_gate[at, :] = both[:, :ff].astype(BF)
        grad_up[at, :] = both[:, ff:].astype(BF)
        grad_down[:, at] = dot(hid_rows[...], rows, ((0,), (0,))).astype(BF)
        return c

    sends = [spread(y, 0, 0, right), spread(y, 1, 1, left), spread(y, 1, 2, right), spread(y, 0, 3, left)]
    for copy in sends:
        copy.start()
    t_row = lax.broadcasted_iota(jnp.int32, (tokens, 1), 0)
    tap = [taps[i : i + 1, :].astype(F32) for i in range(3)]
    gated = c_gate[...].astype(F32) * x_in[...].astype(F32)
    edge_copy(0, 1).wait_recv()
    before = jnp.where(me == 0, 0.0, edge_in[0])
    one_back = jnp.where(t_row == 0, before[7:8], pltpu.roll(gated, 1, 0))
    two_back = jnp.where(
        t_row == 0, before[6:7], jnp.where(t_row == 1, before[7:8], pltpu.roll(gated, 2, 0))
    )
    conv = tap[0] * two_back + tap[1] * one_back + tap[2] * gated
    loads[7].wait()
    b_f = b_gate[...].astype(F32)
    y_short[...] = (b_f * conv).astype(BF)
    loads[8].wait()

    def project(k):
        grad = dot(full[k], y_short[...], ((0,), (0,))).astype(BF)
        for zz in range(2):
            for j in range(PLANE):
                at = (zz * PLANE + j) * out_rows
                outs[j % 2, j // 2, 2 * k + zz] = grad[at : at + out_rows]
        return dot(full[k], w_out[pl.ds(pl.multiple_of(k * share, share), share), :])

    core, x_at = cell % 2, cell // 2
    chips = PLANE // 2

    def to_partner(k):
        return pltpu.make_async_remote_copy(
            outs.at[1 - core, :, pl.ds(2 * k, 2)], pair_in.at[:, pl.ds(2 * k, 2)], p_out.at[k], p_in.at[k],
            device_id=device(z * PLANE + x_at * 2 + 1 - core, y),
        )

    def send_out(k):
        to_partner(k).wait_recv()
        at = pl.ds(2 * k, 2)
        pair_sum[:, at] = (outs[core, :, at].astype(F32) + pair_in[:, at].astype(F32)).astype(BF)
        for j in range(1, chips):
            to = (x_at + j) % chips
            pltpu.make_async_remote_copy(
                pair_sum.at[to, at], outs_in.at[x_at, at], o_out, o_in,
                device_id=device(z * PLANE + to * 2 + core, y),
            ).start()

    d_y = project(y)
    to_partner(y).start()
    lax.fori_loop(0, 1, weight_grads, 0)
    send_out(y)
    spread(left, 0, 0, left).wait_recv()
    sends.append(spread(left, 0, 4, right))
    sends[-1].start()
    spread(right, 1, 1, right).wait_recv()
    sends.append(spread(right, 1, 5, left))
    sends[-1].start()
    spread(left, 1, 2, left).wait_recv()
    d_y += project(left)
    to_partner(left).start()
    spread(right, 0, 3, right).wait_recv()
    d_y += project(right)
    to_partner(right).start()
    send_out(left)
    send_out(right)
    lax.fori_loop(1, 2, weight_grads, 0)
    spread(far, 0, 4, right).wait_recv()
    spread(far, 1, 5, left).wait_recv()
    d_y += project(far)
    to_partner(far).start()
    d_conv = b_f * d_y
    edge[1] = d_conv[0:8]
    small[0] = (d_y * conv).astype(BF)
    edge_copy(1, -1).start()
    send_out(far)
    lax.fori_loop(2, 3, weight_grads, 0)
    edge_copy(1, -1).wait_recv()
    after = jnp.where(me == SP - 1, 0.0, edge_in[1])
    one_on = jnp.where(t_row == tokens - 1, after[0:1], pltpu.roll(d_conv, tokens - 1, 0))
    two_on = jnp.where(
        t_row == tokens - 2,
        after[0:1],
        jnp.where(t_row == tokens - 1, after[1:2], pltpu.roll(d_conv, tokens - 2, 0)),
    )
    d_v = tap[2] * d_conv + tap[1] * one_on + tap[0] * two_on
    small[1] = (d_v * x_in[...].astype(F32)).astype(BF)
    small[2] = (d_v * c_gate[...].astype(F32)).astype(BF)
    wait_bytes(outs_in.at[pl.ds(0, chips - 1)], o_in)

    def sum_plane(p, c):
        acc = pair_sum[x_at, p].astype(F32)
        for j in range(1, chips):
            acc += outs_in[(x_at + j) % chips, p].astype(F32)
        plane_sum[p] = acc.astype(BF)
        return c

    lax.fori_loop(0, PLANES, sum_plane, 0)

    def send_sum(i, c):
        to = (z + i) % PLANES
        pltpu.make_async_remote_copy(
            plane_sum.at[to], plane_in.at[z], q_out, q_in, device_id=device(to * PLANE + cell, y)
        ).start()
        return c

    lax.fori_loop(1, PLANES, send_sum, 0)
    lax.fori_loop(3, 4, weight_grads, 0)
    wait_bytes(plane_in.at[pl.ds(0, PLANES - 1)], q_in)
    acc = plane_sum[z].astype(F32)
    for i in range(1, PLANES):
        acc += plane_in[(z + i) % PLANES].astype(F32)
    grad_out[...] = acc

    wait_bytes(got.at[0, pl.ds(0, len(FAR) * PLANE)], z_out)
    for n in range(len(NEAR)):
        wait_bytes(full_blocks(n), f_out.at[n])
    for k in range(4):
        wait_bytes(got.at[0, pl.ds(0, (PLANE if k < 2 else mid) * len(FAR))], y_out.at[k])
    for k in range(2):
        wait_bytes(part.at[0, pl.ds(0, SP // 2)], a_out.at[k])
        wait_bytes(part.at[0], b_out.at[k])
        edge_copy(k, 1).wait_send()
    wait_bytes(part.at[0, pl.ds(0, SP - 1)], r_out)
    for copy in sends:
        copy.wait_send()
    wait_bytes(outs_in.at[pl.ds(0, chips - 1)], o_out)
    for k in range(TP):
        to_partner(k).wait_send()
    wait_bytes(plane_in.at[pl.ds(0, PLANES - 1)], q_out)


def store_kernel(*refs):
    results, (small, *outs), sems = refs[:5], refs[5:-1], refs[-1]
    sources = [*results, small.at[0], small.at[1], small.at[2]]
    copies = [
        pltpu.make_async_copy(a, b, sems.at[i]) for i, (a, b) in enumerate(zip(sources, outs, strict=True))
    ]
    for copy in copies:
        copy.start()
    for copy in copies:
        copy.wait()


def store(*results):
    small = results[-1]
    likes = [jax.ShapeDtypeStruct(a.shape, a.dtype) for a in results[:-1]]
    likes += [jax.ShapeDtypeStruct(small.shape[1:], small.dtype)] * 3
    return pl.pallas_call(
        store_kernel,
        out_shape=likes,
        in_specs=[VMEM] * len(results),
        out_specs=[pl.BlockSpec(memory_space=pltpu.HBM)] * len(likes),
        scratch_shapes=[pltpu.SemaphoreType.DMA((len(likes),))],
        compiler_params=pltpu.CompilerParams(vmem_limit_bytes=8 * 2**20),
        name="store",
    )(*results)


def per_device(
    hidden_in, cotangent, routes, routing_weights, w_gate, w_up, w_down, b_gate, c_gate, x_in, taps, w_out
):
    tokens, width = hidden_in.shape
    share, ff, short = width // TP, w_gate.shape[2], x_in.shape[1]
    half = share // 2
    slots, out_rows = SP * ROWS, width // SP
    like, dma = jax.ShapeDtypeStruct, pltpu.SemaphoreType.DMA
    hbm = pl.BlockSpec(memory_space=pl.ANY)
    outs = pl.pallas_call(
        kernel,
        out_shape=(
            like((width, ff), BF),
            like((width, ff), BF),
            like((ff, width), BF),
            like((out_rows, short), F32),
            like((tokens, share), BF),
            like((3, tokens, short), BF),
        ),
        in_specs=[VMEM] * 3 + [hbm] * 9,
        out_specs=(VMEM,) * 6,
        scratch_shapes=[
            pltpu.VMEM((tokens, width), BF),
            pltpu.VMEM((tokens, width), BF),
            pltpu.VMEM((width, ff), BF),
            pltpu.VMEM((width, ff), BF),
            pltpu.VMEM((ff, width), BF),
            pltpu.VMEM((width, short), BF),
            pltpu.VMEM((tokens, short), BF),
            pltpu.VMEM((tokens, short), BF),
            pltpu.VMEM((tokens, short), BF),
            pltpu.VMEM((SP, ROWS, share), BF),
            pltpu.VMEM((len(NEAR), TP, PLANE, ROWS, share), BF),
            pltpu.VMEM((slots, tokens), BF),
            pltpu.VMEM((TP, SP, ROWS, share), BF),
            pltpu.VMEM((TP, SP, ROWS, half), BF),
            pltpu.VMEM((2, PLANES, PLANE // 2, ROWS, half), BF),
            pltpu.VMEM((2, PLANES, PLANE, ROWS, half), BF),
            pltpu.VMEM((SP, ROWS, half), BF),
            pltpu.VMEM((SP, ROWS, half), BF),
            pltpu.VMEM((slots, 2 * ff), BF),
            pltpu.VMEM((slots, ff), BF),
            pltpu.VMEM((TP, tokens, share), BF),
            pltpu.VMEM((tokens, short), BF),
            pltpu.VMEM((2, 8, short), F32),
            pltpu.VMEM((2, 8, short), F32),
            pltpu.VMEM((2, PLANE // 2, PLANES, out_rows, short), BF),
            pltpu.VMEM((PLANE // 2, PLANES, out_rows, short), BF),
            pltpu.VMEM((PLANE // 2, PLANES, out_rows, short), BF),
            pltpu.VMEM((PLANE // 2, PLANES, out_rows, short), BF),
            pltpu.VMEM((PLANES, out_rows, short), BF),
            pltpu.VMEM((PLANES, out_rows, short), BF),
            dma((9,)),
            dma((PLANES,)),
            dma(()),
            dma((len(NEAR),)),
            dma((len(NEAR),)),
            dma((4, PLANES)),
            dma((4,)),
            dma((2, PLANES)),
            dma((2,)),
            dma((2, PLANES)),
            dma((2,)),
            dma(()),
            dma(()),
            dma((2,)),
            dma((2,)),
            dma((6,)),
            dma((6,)),
            dma((TP,)),
            dma((TP,)),
            dma(()),
            dma(()),
            dma(()),
            dma(()),
        ],
        compiler_params=pltpu.CompilerParams(
            collective_id=0, has_side_effects=True, vmem_limit_bytes=44 * 2**20
        ),
        name="layer",
    )(
        routes.T, routing_weights.T, taps,
        *[
            pltpu.with_memory_space_constraint(v, pltpu.HBM)
            for v in (hidden_in, cotangent, w_gate[0], w_up[0], w_down[0], w_out, b_gate, c_gate, x_in)
        ],
    )
    grad_gate, grad_up, grad_down, *others = store(*outs)
    return grad_gate[None], grad_up[None], grad_down[None], *others


def solution(mesh):
    seq, both = P("sp", None), P("sp", "tp")
    return jax.shard_map(
        per_device,
        mesh=mesh,
        in_specs=(
            seq,
            seq,
            seq,
            seq,
            P("sp", None, "tp"),
            P("sp", None, "tp"),
            P("sp", "tp", None),
            both,
            both,
            both,
            P(None, "tp"),
            P(None, "tp"),
        ),
        out_specs=(
            P("sp", None, "tp"),
            P("sp", None, "tp"),
            P("sp", "tp", None),
            both,
            both,
            both,
            both,
            both,
        ),
        check_vma=False,
    )
```

```python
import functools

import jax
import jax.numpy as jnp
from jax import lax
from jax.experimental import pallas as pl
from jax.experimental.pallas import tpu as pltpu
from jax.sharding import PartitionSpec as P

PLANES, PLANE, TP, CAP = 8, 8, 4, 12
SP = PLANES * PLANE
ROWS = 2 * CAP
VMEM = pl.BlockSpec(memory_space=pltpu.VMEM)
BF, F32 = jnp.bfloat16, jnp.float32


def dot(a, b, dims=((1,), (0,))):
    return lax.dot_general(a, b, (dims, ((), ())), preferred_element_type=F32)


def device(sp, tp):
    return {"sp": sp, "tp": tp}


STEPS = (0, 2, 6, 3, 5, 4, 1, 7)
NEAR = (0, 6, 7)
FAR = range(1, 6)
NEAR_AT = 3
FIRST = 4


def plane_step(g):
    if isinstance(g, int):
        return STEPS[g]
    return sum(jnp.where(g == i, step, 0) for i, step in enumerate(STEPS))


def greet_all(me, y, right, left):
    barrier = pltpu.get_barrier_semaphore()

    def signal(i, c):
        pl.semaphore_signal(barrier, inc=1, device_id=device((me + i) % SP, y))
        return c

    lax.fori_loop(1, SP, signal, 0)
    pl.semaphore_signal(barrier, inc=1, device_id=device(me, right))
    pl.semaphore_signal(barrier, inc=1, device_id=device(me, left))
    return barrier


def wait_bytes(ref, sem):
    pltpu.make_async_copy(ref, ref, sem).wait()


def kernel(
    routes_hbm, weights_hbm, taps_hbm, hidden_hbm, cot_hbm, w_gate_hbm, w_up_hbm, w_down_hbm, w_out_hbm, b_hbm, c_hbm, x_hbm,
    grad_gate, grad_up, grad_down, grad_out, residual, small,
    routes, weights, taps, hidden, cot, w_gate, w_up, w_down, w_out, b_gate, c_gate, x_in,
    send, own, select, got, part, near_in, total_in, sums, back, d_both, hid_rows, full, y_short,
    edge, edge_in, outs, pair_in, pair_sum, outs_in, plane_sum, plane_in,
    ld, z_in, z_out, f_in, f_out, y_in, y_out, a_in, a_out, b_in, b_out, r_in, r_out,
    h_in, h_out, e_in, e_out, p_in, p_out, o_in, o_out, q_in, q_out,
):
    me, y = lax.axis_index("sp"), lax.axis_index("tp")
    z, cell = me // PLANE, me % PLANE
    right, left, far = (y + 1) % TP, (y + 3) % TP, (y + 2) % TP
    tokens, width = hidden.shape
    share = width // TP
    half_share = share // 2
    part_rows = PLANE * ROWS
    slots = SP * ROWS
    mid = PLANE // 2
    ff = w_gate.shape[1]
    out_rows = grad_out.shape[0]

    loads = [
        pltpu.make_async_copy(a, b, ld.at[i])
        for i, (a, b) in enumerate(
            (
                (routes_hbm, routes),
                (weights_hbm, weights),
                (hidden_hbm, hidden),
                (cot_hbm, cot),
                (c_hbm, c_gate),
                (x_hbm, x_in),
                (w_gate_hbm, w_gate),
                (w_up_hbm, w_up),
                (w_down_hbm, w_down),
                (b_hbm, b_gate),
                (w_out_hbm, w_out),
                (taps_hbm, taps),
            )
        )
    ]
    for load in loads[:FIRST]:
        load.start()
    barrier = greet_all(me, y, right, left)
    for load in loads[FIRST:]:
        load.start()

    down = lax.broadcasted_iota(jnp.int32, (tokens, tokens), 0)
    across = lax.broadcasted_iota(jnp.int32, (tokens, tokens), 1)

    def count(match):
        return jnp.sum(jnp.where(match, 1.0, 0.0), axis=0, keepdims=True).astype(jnp.int32)

    loads[0].wait()
    loads[1].wait()
    r0, r1 = routes[0:1, :], routes[1:2, :]
    w0, w1 = weights[0:1, :], weights[1:2, :]
    c0 = jnp.sum(jnp.where(down == across, r0, 0), axis=1, keepdims=True)
    c1 = jnp.sum(jnp.where(down == across, r1, 0), axis=1, keepdims=True)
    earlier = down < across
    t0 = r0 * ROWS + count(earlier & (c0 == r0))
    t1 = r1 * ROWS + count(c0 == r1) + count(earlier & (c1 == r1))
    row = lax.broadcasted_iota(jnp.int32, (part_rows, tokens), 0)
    is_token = lax.broadcasted_iota(jnp.int32, (part_rows, 1), 0) % ROWS < CAP

    def picks(plane):
        slot = row + plane * part_rows
        h = jnp.where((t0 == slot) | (t1 == slot), 1.0, 0.0)
        s0, s1 = t0 + CAP == slot, t1 + CAP == slot
        s = jnp.where(s0 | s1, 1.0, 0.0)
        scale = jnp.sum(jnp.where(s0, w0, 0.0) + jnp.where(s1, w1, 0.0), axis=1, keepdims=True)
        select[pl.ds(pl.multiple_of(plane * part_rows, part_rows), part_rows), :] = (h + s).astype(BF)
        return h.astype(BF), s.astype(BF), jnp.where(is_token, 1.0, scale)

    def plane_of(g, sign):
        return (z + sign * plane_step(g) + PLANES) % PLANES

    mine = pl.ds(pl.multiple_of(y * share, share), share)

    def pack(g):
        plane = plane_of(g, 1)
        h, s, scale = picks(plane)
        rows = (dot(h, hidden[:, mine]) + dot(s, cot[:, mine])) * scale
        send[pl.ds(plane * PLANE, PLANE)] = rows.astype(BF).reshape(PLANE, ROWS, share)

    def send_group(g):
        def one(j, c):
            to = plane_of(g, 1) * PLANE + (cell + j) % PLANE
            pltpu.make_async_remote_copy(
                send.at[to], got.at[y, me], z_out, z_in.at[g], device_id=device(to, y)
            ).start()
            return c

        lax.fori_loop(0, PLANE, one, 0)

    loads[2].wait()
    loads[3].wait()
    def pack_full(n):
        plane = plane_of(NEAR[n], 1)
        h, s, scale = picks(plane)
        for k in range(TP):
            cols = pl.ds(k * share, share)
            rows = (dot(h, hidden[:, cols]) + dot(s, cot[:, cols])) * scale
            own[n, k] = rows.astype(BF).reshape(PLANE, ROWS, share)

    def send_full(n, first):
        count = PLANE - first

        def one(i, c):
            j, k = (cell + first + i % count) % PLANE, i // count
            to = plane_of(NEAR[n], 1) * PLANE + j
            pltpu.make_async_remote_copy(
                own.at[n, k, j], got.at[k, me], f_out.at[n], f_in.at[n], device_id=device(to, y)
            ).start()
            return c

        lax.fori_loop(0, TP * count, one, 0)

    lax.fori_loop(1, 3, lambda g, c: (pack(g), c)[1], 0)
    pl.semaphore_wait(barrier, SP + 1)
    lax.fori_loop(1, 3, lambda g, c: (send_group(g), c)[1], 0)
    lax.fori_loop(3, FAR[-1] + 1, lambda g, c: (pack(g), c)[1], 0)
    pack_full(0)
    for k in range(TP):
        got[k, me] = own[0, k, cell]
    lax.fori_loop(3, FAR[-1] + 1, lambda g, c: (send_group(g), c)[1], 0)
    send_full(0, 1)
    pack_full(1)
    pack_full(2)

    loads[4].wait()
    loads[5].wait()
    edge[0] = c_gate[tokens - 8 :, :].astype(F32) * x_in[tokens - 8 :, :].astype(F32)

    def edge_copy(k, by):
        return pltpu.make_async_remote_copy(
            edge.at[k], edge_in.at[k], h_out.at[k], h_in.at[k], device_id=device((me + by + SP) % SP, y)
        )

    edge_copy(0, 1).start()
    for load in loads[6:9]:
        load.wait()

    def block(k, g, at=0, size=PLANE):
        return got.at[k, pl.ds(plane_of(g, -1) * PLANE + at, size)]

    def pass_on(s, g, k, to):
        ref = block(s, g) if k < 2 else block(s, g, (k - 2) * mid, mid)
        return pltpu.make_async_remote_copy(
            ref, ref, y_out.at[k], y_in.at[k, g], device_id=device(me, to)
        )

    def expert_rows(g):
        plane = plane_of(g, -1)
        blocks = pl.ds(plane * PLANE, PLANE)
        pre_gate = pre_up = d_hid = jnp.zeros((part_rows, ff), F32)
        for k in range(TP):
            x = got[k, blocks].reshape(part_rows, share)
            cols = pl.ds(k * share, share)
            pre_gate += dot(x, w_gate[cols, :])
            pre_up += dot(x, w_up[cols, :])
            d_hid += dot(x, w_down[:, cols], ((1,), (1,)))
        d_hid = pltpu.roll(d_hid, part_rows - CAP, 0)
        sigma = 1.0 / (1.0 + jnp.exp(-pre_gate))
        silu = pre_gate * sigma
        d_up = d_hid * silu
        d_pre = d_hid * pre_up * sigma * (1.0 + pre_gate * (1.0 - sigma))
        twice_pre = jnp.where(is_token, d_pre, pltpu.roll(d_pre, CAP, 0)).astype(BF)
        twice_up = jnp.where(is_token, d_up, pltpu.roll(d_up, CAP, 0)).astype(BF)
        for k in range(TP):
            cols = pl.ds(k * share, share)
            grad = dot(twice_pre, w_gate[cols, :], ((1,), (1,)))
            grad += dot(twice_up, w_up[cols, :], ((1,), (1,)))
            folded = jnp.where(is_token, grad[:, :half_share], grad[:, half_share:])
            part[k, blocks] = folded.astype(BF).reshape(PLANE, ROWS, half_share)
        at = pl.ds(pl.multiple_of(plane * part_rows, part_rows), part_rows)
        d_both[at, 0:ff] = jnp.where(is_token, d_pre, 0.0).astype(BF)
        d_both[at, ff:] = jnp.where(is_token, d_up, 0.0).astype(BF)
        hid_rows[at, :] = jnp.where(is_token, 0.0, pltpu.roll(silu * pre_up, CAP, 0)).astype(BF)

    def far_half(g, k, to):
        at = plane_of(g, -1) * PLANE + k * mid
        return pltpu.make_async_remote_copy(
            part.at[far, pl.ds(at, mid)], near_in.at[k, g], a_out.at[k], a_in.at[k, g],
            device_id=device(me, to),
        )

    def near_sum(g, k, to):
        return pltpu.make_async_remote_copy(
            part.at[to, pl.ds(plane_of(g, -1) * PLANE, PLANE)], total_in.at[k, g], b_out.at[k],
            b_in.at[k, g], device_id=device(me, to),
        )

    def add(g, k, to):
        at = pl.ds(plane_of(g, -1) * PLANE + k * mid, mid)
        part[to, at] = (part[to, at].astype(F32) + near_in[k, g].astype(F32)).astype(BF)

    def send_back(g, j):
        to = plane_of(g, -1) * PLANE + (cell + j) % PLANE
        pltpu.make_async_remote_copy(
            sums.at[to], back.at[me], r_out, r_in, device_id=device(to, y)
        ).start()

    def full_blocks(n):
        return got.at[0, pl.ds(0, TP * (PLANE - 1 if n == 0 else PLANE))]

    def step(t, c):
        @pl.when(t == NEAR_AT)
        def _():
            send_full(1, 0)
            send_full(2, 0)

        @pl.when(t <= FAR[-1])
        def _():
            wait_bytes(block(y, t), z_in.at[t])
            pass_on(y, t, 0, right).start()
            pass_on(y, t, 1, left).start()

        @pl.when((t > 1) & (t <= FAR[-1] + 1))
        def _():
            g = t - 1
            pass_on(left, g, 0, left).wait_recv()
            pass_on(left, g, 2, right).start()
            pass_on(right, g, 1, right).wait_recv()
            pass_on(right, g, 3, left).start()

        @pl.when((t >= 4) & (t < PLANES + 4))
        def _():
            g = t - 4
            far_half(g, 0, right).wait_recv()
            add(g, 0, right)
            far_half(g, 1, left).wait_recv()
            add(g, 1, left)

        @pl.when(t >= 6)
        def _():
            g = t - 6

            @pl.when(g > 0)
            def _():
                send_back(g, 0)

            lax.fori_loop(1, PLANE, lambda j, d: (send_back(g, j), d)[1], 0)

        @pl.when((t >= 4) & (t < PLANES + 4))
        def _():
            near_sum(t - 4, 0, right).start()
            near_sum(t - 4, 1, left).start()

        @pl.when((t >= 5) & (t < PLANES + 5))
        def _():
            g = t - 5
            near_sum(g, 0, right).wait_recv()
            near_sum(g, 1, left).wait_recv()
            at = pl.ds(plane_of(g, -1) * PLANE, PLANE)
            sums[at] = (
                part[y, at].astype(F32) + total_in[0, g].astype(F32) + total_in[1, g].astype(F32)
            ).astype(BF)

        for n, g in enumerate(NEAR):

            @pl.when(t == g + 2)
            def _():
                wait_bytes(full_blocks(n), f_in.at[n])

        @pl.when((t > 2) & (t <= FAR[-1] + 2))
        def _():
            pass_on(far, t - 2, 2, right).wait_recv()
            pass_on(far, t - 2, 3, left).wait_recv()

        @pl.when((t >= 2) & (t < PLANES + 2))
        def _():
            expert_rows(t - 2)
            far_half(t - 2, 0, right).start()
            far_half(t - 2, 1, left).start()

        return c

    lax.fori_loop(1, PLANES + 6, step, 0)
    back[me] = sums[me]

    wait_bytes(part.at[0, pl.ds(0, SP - 1)], r_in)
    token_slot = lax.broadcasted_iota(jnp.int32, (slots, 1), 0) % ROWS < CAP
    rows = back[...].reshape(slots, half_share)
    zero = jnp.zeros_like(rows)
    kept = jnp.concatenate(
        [jnp.where(token_slot, rows, zero), jnp.where(token_slot, zero, rows)], axis=1
    )
    total = (cot[:, mine].astype(F32) + dot(select[...], kept, ((0,), (0,)))).astype(BF)
    full[y] = total
    residual[...] = total

    rows_half = tokens // 2

    def spread(s, at, k, to):
        ref = full.at[s, pl.ds(at * rows_half, rows_half)]
        return pltpu.make_async_remote_copy(
            ref, ref, e_out.at[k], e_in.at[k], device_id=device(me, to)
        )

    def weight_grads(k, c):
        rows = got[k].reshape(slots, share)
        at = pl.ds(pl.multiple_of(k * share, share), share)
        both = dot(rows, d_both[...], ((0,), (0,)))
        grad_gate[at, :] = both[:, :ff].astype(BF)
        grad_up[at, :] = both[:, ff:].astype(BF)
        grad_down[:, at] = dot(hid_rows[...], rows, ((0,), (0,))).astype(BF)
        return c

    sends = [spread(y, 0, 0, right), spread(y, 1, 1, left), spread(y, 1, 2, right), spread(y, 0, 3, left)]
    for copy in sends:
        copy.start()
    t_row = lax.broadcasted_iota(jnp.int32, (tokens, 1), 0)
    loads[11].wait()
    tap = [taps[i : i + 1, :].astype(F32) for i in range(3)]
    gated = c_gate[...].astype(F32) * x_in[...].astype(F32)
    edge_copy(0, 1).wait_recv()
    before = jnp.where(me == 0, 0.0, edge_in[0])
    one_back = jnp.where(t_row == 0, before[7:8], pltpu.roll(gated, 1, 0))
    two_back = jnp.where(
        t_row == 0, before[6:7], jnp.where(t_row == 1, before[7:8], pltpu.roll(gated, 2, 0))
    )
    conv = tap[0] * two_back + tap[1] * one_back + tap[2] * gated
    loads[9].wait()
    b_f = b_gate[...].astype(F32)
    y_short[...] = (b_f * conv).astype(BF)
    loads[10].wait()

    def project(k):
        grad = dot(full[k], y_short[...], ((0,), (0,))).astype(BF)
        for zz in range(2):
            for j in range(PLANE):
                at = (zz * PLANE + j) * out_rows
                outs[j % 2, j // 2, 2 * k + zz] = grad[at : at + out_rows]
        return dot(full[k], w_out[pl.ds(pl.multiple_of(k * share, share), share), :])

    core, x_at = cell % 2, cell // 2
    chips = PLANE // 2

    def to_partner(k):
        return pltpu.make_async_remote_copy(
            outs.at[1 - core, :, pl.ds(2 * k, 2)], pair_in.at[:, pl.ds(2 * k, 2)], p_out.at[k], p_in.at[k],
            device_id=device(z * PLANE + x_at * 2 + 1 - core, y),
        )

    def send_out(k):
        to_partner(k).wait_recv()
        at = pl.ds(2 * k, 2)
        pair_sum[:, at] = (outs[core, :, at].astype(F32) + pair_in[:, at].astype(F32)).astype(BF)
        for j in range(1, chips):
            to = (x_at + j) % chips
            pltpu.make_async_remote_copy(
                pair_sum.at[to, at], outs_in.at[x_at, at], o_out, o_in,
                device_id=device(z * PLANE + to * 2 + core, y),
            ).start()

    d_y = project(y)
    to_partner(y).start()
    lax.fori_loop(0, 1, weight_grads, 0)
    send_out(y)
    spread(left, 0, 0, left).wait_recv()
    sends.append(spread(left, 0, 4, right))
    sends[-1].start()
    spread(right, 1, 1, right).wait_recv()
    sends.append(spread(right, 1, 5, left))
    sends[-1].start()
    spread(left, 1, 2, left).wait_recv()
    d_y += project(left)
    to_partner(left).start()
    spread(right, 0, 3, right).wait_recv()
    d_y += project(right)
    to_partner(right).start()
    send_out(left)
    send_out(right)
    lax.fori_loop(1, 2, weight_grads, 0)
    spread(far, 0, 4, right).wait_recv()
    spread(far, 1, 5, left).wait_recv()
    d_y += project(far)
    to_partner(far).start()
    d_conv = b_f * d_y
    edge[1] = d_conv[0:8]
    small[0] = (d_y * conv).astype(BF)
    edge_copy(1, -1).start()
    send_out(far)
    lax.fori_loop(2, 3, weight_grads, 0)
    edge_copy(1, -1).wait_recv()
    after = jnp.where(me == SP - 1, 0.0, edge_in[1])
    one_on = jnp.where(t_row == tokens - 1, after[0:1], pltpu.roll(d_conv, tokens - 1, 0))
    two_on = jnp.where(
        t_row == tokens - 2,
        after[0:1],
        jnp.where(t_row == tokens - 1, after[1:2], pltpu.roll(d_conv, tokens - 2, 0)),
    )
    d_v = tap[2] * d_conv + tap[1] * one_on + tap[0] * two_on
    small[1] = (d_v * x_in[...].astype(F32)).astype(BF)
    small[2] = (d_v * c_gate[...].astype(F32)).astype(BF)
    wait_bytes(outs_in.at[pl.ds(0, chips - 1)], o_in)

    def sum_plane(p, c):
        acc = pair_sum[x_at, p].astype(F32)
        for j in range(1, chips):
            acc += outs_in[(x_at + j) % chips, p].astype(F32)
        plane_sum[p] = acc.astype(BF)
        return c

    lax.fori_loop(0, PLANES, sum_plane, 0)

    def send_sum(i, c):
        to = (z + i) % PLANES
        pltpu.make_async_remote_copy(
            plane_sum.at[to], plane_in.at[z], q_out, q_in, device_id=device(to * PLANE + cell, y)
        ).start()
        return c

    lax.fori_loop(1, PLANES, send_sum, 0)
    lax.fori_loop(3, 4, weight_grads, 0)
    wait_bytes(plane_in.at[pl.ds(0, PLANES - 1)], q_in)
    acc = plane_sum[z].astype(F32)
    for i in range(1, PLANES):
        acc += plane_in[(z + i) % PLANES].astype(F32)
    grad_out[...] = acc

    wait_bytes(got.at[0, pl.ds(0, len(FAR) * PLANE)], z_out)
    for n in range(len(NEAR)):
        wait_bytes(full_blocks(n), f_out.at[n])
    for k in range(4):
        wait_bytes(got.at[0, pl.ds(0, (PLANE if k < 2 else mid) * len(FAR))], y_out.at[k])
    for k in range(2):
        wait_bytes(part.at[0, pl.ds(0, SP // 2)], a_out.at[k])
        wait_bytes(part.at[0], b_out.at[k])
        edge_copy(k, 1).wait_send()
    wait_bytes(part.at[0, pl.ds(0, SP - 1)], r_out)
    for copy in sends:
        copy.wait_send()
    wait_bytes(outs_in.at[pl.ds(0, chips - 1)], o_out)
    for k in range(TP):
        to_partner(k).wait_send()
    wait_bytes(plane_in.at[pl.ds(0, PLANES - 1)], q_out)


def store_kernel(*refs):
    results, (small, *outs), sems = refs[:5], refs[5:-1], refs[-1]
    sources = [*results, small.at[0], small.at[1], small.at[2]]
    copies = [
        pltpu.make_async_copy(a, b, sems.at[i]) for i, (a, b) in enumerate(zip(sources, outs, strict=True))
    ]
    for copy in copies:
        copy.start()
    for copy in copies:
        copy.wait()


def store(*results):
    small = results[-1]
    likes = [jax.ShapeDtypeStruct(a.shape, a.dtype) for a in results[:-1]]
    likes += [jax.ShapeDtypeStruct(small.shape[1:], small.dtype)] * 3
    return pl.pallas_call(
        store_kernel,
        out_shape=likes,
        in_specs=[VMEM] * len(results),
        out_specs=[pl.BlockSpec(memory_space=pltpu.HBM)] * len(likes),
        scratch_shapes=[pltpu.SemaphoreType.DMA((len(likes),))],
        compiler_params=pltpu.CompilerParams(vmem_limit_bytes=8 * 2**20),
        name="store",
    )(*results)


def per_device(
    hidden_in, cotangent, routes, routing_weights, w_gate, w_up, w_down, b_gate, c_gate, x_in, taps, w_out
):
    tokens, width = hidden_in.shape
    share, ff, short = width // TP, w_gate.shape[2], x_in.shape[1]
    half = share // 2
    slots, out_rows = SP * ROWS, width // SP
    like, dma = jax.ShapeDtypeStruct, pltpu.SemaphoreType.DMA
    hbm = pl.BlockSpec(memory_space=pl.ANY)
    outs = pl.pallas_call(
        kernel,
        out_shape=(
            like((width, ff), BF),
            like((width, ff), BF),
            like((ff, width), BF),
            like((out_rows, short), F32),
            like((tokens, share), BF),
            like((3, tokens, short), BF),
        ),
        in_specs=[hbm] * 12,
        out_specs=(VMEM,) * 6,
        scratch_shapes=[
            pltpu.VMEM((2, tokens), jnp.int32),
            pltpu.VMEM((2, tokens), F32),
            pltpu.VMEM((3, short), BF),
            pltpu.VMEM((tokens, width), BF),
            pltpu.VMEM((tokens, width), BF),
            pltpu.VMEM((width, ff), BF),
            pltpu.VMEM((width, ff), BF),
            pltpu.VMEM((ff, width), BF),
            pltpu.VMEM((width, short), BF),
            pltpu.VMEM((tokens, short), BF),
            pltpu.VMEM((tokens, short), BF),
            pltpu.VMEM((tokens, short), BF),
            pltpu.VMEM((SP, ROWS, share), BF),
            pltpu.VMEM((len(NEAR), TP, PLANE, ROWS, share), BF),
            pltpu.VMEM((slots, tokens), BF),
            pltpu.VMEM((TP, SP, ROWS, share), BF),
            pltpu.VMEM((TP, SP, ROWS, half), BF),
            pltpu.VMEM((2, PLANES, PLANE // 2, ROWS, half), BF),
            pltpu.VMEM((2, PLANES, PLANE, ROWS, half), BF),
            pltpu.VMEM((SP, ROWS, half), BF),
            pltpu.VMEM((SP, ROWS, half), BF),
            pltpu.VMEM((slots, 2 * ff), BF),
            pltpu.VMEM((slots, ff), BF),
            pltpu.VMEM((TP, tokens, share), BF),
            pltpu.VMEM((tokens, short), BF),
            pltpu.VMEM((2, 8, short), F32),
            pltpu.VMEM((2, 8, short), F32),
            pltpu.VMEM((2, PLANE // 2, PLANES, out_rows, short), BF),
            pltpu.VMEM((PLANE // 2, PLANES, out_rows, short), BF),
            pltpu.VMEM((PLANE // 2, PLANES, out_rows, short), BF),
            pltpu.VMEM((PLANE // 2, PLANES, out_rows, short), BF),
            pltpu.VMEM((PLANES, out_rows, short), BF),
            pltpu.VMEM((PLANES, out_rows, short), BF),
            dma((12,)),
            dma((PLANES,)),
            dma(()),
            dma((len(NEAR),)),
            dma((len(NEAR),)),
            dma((4, PLANES)),
            dma((4,)),
            dma((2, PLANES)),
            dma((2,)),
            dma((2, PLANES)),
            dma((2,)),
            dma(()),
            dma(()),
            dma((2,)),
            dma((2,)),
            dma((6,)),
            dma((6,)),
            dma((TP,)),
            dma((TP,)),
            dma(()),
            dma(()),
            dma(()),
            dma(()),
        ],
        compiler_params=pltpu.CompilerParams(
            collective_id=0, has_side_effects=True, vmem_limit_bytes=44 * 2**20
        ),
        name="layer",
    )(
        *[
            pltpu.with_memory_space_constraint(v, pltpu.HBM)
            for v in (routes.T, routing_weights.T, taps, hidden_in, cotangent, w_gate[0], w_up[0], w_down[0], w_out, b_gate, c_gate, x_in)
        ],
    )
    grad_gate, grad_up, grad_down, *others = store(*outs)
    return grad_gate[None], grad_up[None], grad_down[None], *others


def solution(mesh):
    seq, both = P("sp", None), P("sp", "tp")
    return jax.shard_map(
        per_device,
        mesh=mesh,
        in_specs=(
            seq,
            seq,
            seq,
            seq,
            P("sp", None, "tp"),
            P("sp", None, "tp"),
            P("sp", "tp", None),
            both,
            both,
            both,
            P(None, "tp"),
            P(None, "tp"),
        ),
        out_specs=(
            P("sp", None, "tp"),
            P("sp", None, "tp"),
            P("sp", "tp", None),
            both,
            both,
            both,
            both,
            both,
        ),
        check_vma=False,
    )
```
